32 devices in a mesh: ra: 8 (over z, y), cb: 4 (over x, core).
Axes of the slice: x: 2, y: 2, z: 4, core: 2. Of those that a mesh axis runs over, the one named last changes fastest.
Arguments:
- tokens: bfloat16 [1024, 4096], P(None, 'ra'), may hold values from -40 to 40
- norm_gain: float32 [4096], P('ra'), may hold values from 0.1 to 1.9
- gate_weight: bfloat16 [4096, 11264], P('ra', 'cb'), may hold values from -0.09375 to 0.09375
- up_weight: bfloat16 [4096, 11264], P('ra', 'cb'), may hold values from -0.09375 to 0.09375
- down_weight: bfloat16 [11264, 4096], P('cb', 'ra'), may hold values from -0.0546875 to 0.0546875
- out_gain: float32 [4096], P('ra'), may hold values from 0.1 to 1.9
Outputs:
- normed: bfloat16 [1024, 4096], P(None, 'ra')
The draws below stay inside these ranges and needn't reach their ends.
All inputs are finite; a program needn't handle non-finite values.
Results may differ from the reference program's by a relative error of at most 0.0076.
Values may be sent and summed in bfloat16 or wider, within the bound.
A program may use at most 128 MiB of HBM per device.

```python
import jax
import jax.numpy as jnp
from jax import lax

D = 4096
FF = 11264
TOKENS = 1024


def draw_tokens(key, part):
    keys = jax.random.split(key, 4)
    base = jax.random.normal(keys[0], (TOKENS, D), jnp.float32)
    blocks = jnp.exp(jax.random.uniform(keys[1], (16,), jnp.float32, jnp.log(0.3), jnp.log(3.0)))
    columns = jnp.repeat(blocks, D // 16)[None, :]
    rows = jax.random.uniform(keys[2], (TOKENS, 1), jnp.float32, 0.5, 2.0)
    return jnp.clip(base * columns * rows, -40.0, 40.0).astype(jnp.bfloat16)


def block_scale(key, dims, cuts, smallest, high):
    factor_of = 1.0
    for dim, blocks in cuts:
        heights = jax.random.uniform(jax.random.fold_in(jax.random.fold_in(key, 6), dim), (blocks,), jnp.float32, smallest / len(cuts), high / len(cuts))
        factor_of = factor_of * jnp.repeat(jnp.exp(heights), dims[dim] // blocks).reshape((-1,) + (1,) * (len(dims) - 1 - dim))
    return factor_of


def gaussian(rng, dims, deviation, bound, cuts=(), kind=jnp.bfloat16):
    entries = deviation * jax.random.normal(rng, dims, jnp.float32)
    if cuts:
        entries = entries * block_scale(rng, dims, cuts, -0.22, 0.18)
    return jnp.clip(entries, -bound, bound).astype(kind)


def setup_inputs(seed: int = 0) -> dict:
    key_list = jax.random.split(jax.random.key(seed), 7)
    return {
        "tokens": draw_tokens(jax.random.fold_in(key_list[6], 71), 0),
        "norm_gain": jnp.clip(1.0 + 0.18 * jax.random.normal(key_list[1], (D,), jnp.float32), 0.1, 1.9),
        "gate_weight": gaussian(key_list[2], (D, FF), D ** -0.5, 0.09375, ((0, 8), (1, 4))),
        "up_weight": gaussian(key_list[3], (D, FF), D ** -0.5, 0.09375, ((0, 8), (1, 4))),
        "down_weight": gaussian(key_list[4], (FF, D), FF ** -0.5, 0.0546875, ((0, 4), (1, 8))),
        "out_gain": jnp.clip(1.0 + 0.18 * jax.random.normal(key_list[5], (D,), jnp.float32), 0.1, 1.9),
    }


def reference(tokens, norm_gain, gate_weight, up_weight, down_weight, out_gain):
    stream_in = tokens.astype(jnp.float32)
    inv_rms = jax.lax.rsqrt(lax.optimization_barrier(jnp.sum(stream_in * stream_in, axis=1)) / D + 1e-06)[:, None]
    scaled = (stream_in * norm_gain[None, :]).astype(jnp.bfloat16)
    gate = jnp.dot(scaled, gate_weight, preferred_element_type=jnp.float32) * inv_rms
    up = jnp.dot(scaled, up_weight, preferred_element_type=jnp.float32) * inv_rms
    hidden = (jax.nn.silu(gate) * up).astype(jnp.bfloat16)
    branch = jnp.dot(hidden, down_weight, preferred_element_type=jnp.float32)
    stream = 0.5 * stream_in + branch
    factor = jax.lax.rsqrt(lax.optimization_barrier(jnp.sum(stream * stream, axis=1)) / D + 1e-06)[:, None]
    return (stream * factor * out_gain[None, :]).astype(jnp.bfloat16)
```

```python
import functools

import jax
import jax.numpy as jnp
from jax import lax
from jax.experimental import pallas as pl
from jax.experimental.pallas import tpu as pltpu
from jax.sharding import PartitionSpec as P

F32, BF16 = jnp.float32, jnp.bfloat16
MESH = pl.DeviceIdType.MESH
LANES = 128
SUBBLOCKS = 4
EPS = 1e-06


def plane_sizes(mesh):
    n = mesh.shape["ra"]
    column = mesh.devices[:, 0]
    coords = [getattr(d, "coords", None) for d in column]
    if all(c is not None for c in coords):
        ny = len({c[1] for c in coords})
    else:
        ny = 2 if n % 2 == 0 else 1
    return n // ny, ny


def ring_order(mesh):
    n = mesh.shape["ra"]
    column = mesh.devices[:, 0]
    coords = [getattr(d, "coords", None) for d in column]
    if all(c is not None for c in coords):
        ny = len({c[1] for c in coords})
    else:
        ny = 2 if n % 2 == 0 else 1
    nz = n // ny
    if ny == 1 or nz % 2 or nz * ny != n:
        return list(range(n))
    walk = []
    for z in range(nz):
        ys = range(1, ny) if z % 2 == 0 else range(ny - 1, 0, -1)
        walk += [z * ny + y for y in ys]
    return walk + [z * ny for z in reversed(range(nz))]


def butterfly(value, axis, n, narrow=None):
    if n & (n - 1):
        return lax.psum(value, axis)
    step = 1
    while step < n:
        sent = value if narrow is None else value.astype(narrow)
        got = lax.ppermute(sent, axis, [(i, i ^ step) for i in range(n)])
        value = sent.astype(F32) + got.astype(F32)
        step *= 2
    return value


def ring_body(mesh):
    n_ra, n_cb = mesh.shape["ra"], mesh.shape["cb"]
    order = ring_order(mesh)
    place = [order.index(i) for i in range(n_ra)]
    to_right = [(order[i], order[(i + 1) % n_ra]) for i in range(n_ra)]
    to_left = [(order[i], order[(i - 1) % n_ra]) for i in range(n_ra)]
    far = n_ra // 2

    def body(tokens, norm_gain, gate_weight, up_weight, down_weight, out_gain):
        rows = tokens.shape[0] // n_ra
        width = tokens.shape[1] * n_ra
        hidden_cols = gate_weight.shape[1]
        cut = -(-hidden_cols // 256) * 128
        cols = (slice(0, cut), slice(cut, hidden_cols))
        p = jnp.asarray(place, jnp.int32)[lax.axis_index("ra")]

        def block(array, b):
            start = lax.rem(p + b + n_ra, n_ra) * rows
            return lax.dynamic_slice_in_dim(array, start, rows, 0)

        stream_in = tokens.astype(F32)
        scaled = (stream_in * norm_gain[None, :]).astype(BF16)
        weights = {"g": gate_weight, "u": up_weight}

        def parts(source, offsets):
            x = jnp.concatenate([block(source, b) for b in offsets], axis=0)
            return {k: jnp.dot(x, w, preferred_element_type=F32) for k, w in weights.items()}

        right, left = {}, {}
        source = scaled
        for d in range(far, 0, -1):
            mine = parts(source, (d,) if d == far else (d, -d))
            if d < far:
                source, right["g"] = lax.optimization_barrier((source, right["g"]))
            for key in ("g", "u"):
                for flow, perm, skip, at in ((right, to_right, "u", 0), (left, to_left, "g", rows)):
                    if d == far and key == skip:
                        continue
                    value = mine[key] if d == far else mine[key][at : at + rows]
                    if key in flow:
                        value = value + flow[key].astype(F32)
                    flow[key] = lax.ppermute(value.astype(BF16), "ra", perm)
        mine = parts(source, (0,))

        squares = jnp.sum(stream_in * stream_in, axis=1)
        sq = block(squares, 0)
        for k in range(1, n_ra):
            perm = [(order[i], order[(i + k) % n_ra]) for i in range(n_ra)]
            sq = sq + lax.ppermute(block(squares, k), "ra", perm)
        inv_rms = lax.rsqrt(sq / width + 1e-06)[:, None]

        total = {}
        for key in ("g", "u"):
            value = mine[key]
            for flow in (right, left):
                if key in flow:
                    value = value + flow[key].astype(F32)
            total[key] = value * inv_rms
        own = (jax.nn.silu(total["g"]) * total["u"]).astype(BF16)

        stream = jnp.zeros(tokens.shape, F32)
        sums = jnp.zeros(tokens.shape[:1], F32)

        def finish(stream, sums, held):
            units = jnp.concatenate([h for _, h in held], axis=0)
            down = jnp.dot(units, down_weight, preferred_element_type=F32)
            branch = butterfly(down, "cb", n_cb, BF16)
            for i, (b, _) in enumerate(held):
                new = 0.5 * block(stream_in, b) + branch[i * rows : (i + 1) * rows]
                start = lax.rem(p + b + n_ra, n_ra) * rows
                stream = lax.dynamic_update_slice_in_dim(stream, new, start, 0)
                sums = lax.dynamic_update_slice_in_dim(sums, jnp.sum(new * new, axis=1), start, 0)
            return stream, sums

        from_left = from_right = own
        pending = [(0, own)]
        for s in range(1, far + 1):
            last = s == far
            if last:
                from_left, from_right = from_left[:, cols[0]], from_right[:, cols[1]]
            from_left = lax.ppermute(from_left, "ra", to_right)
            from_right = lax.ppermute(from_right, "ra", to_left)
            stream, sums = finish(stream, sums, pending)
            if last:
                pending = [(far, jnp.concatenate([from_left, from_right], axis=1))]
            else:
                pending = [(-s, from_left), (s, from_right)]
        stream, sums = finish(stream, sums, pending)

        total_sq = butterfly(sums, "ra", n_ra)
        factor = lax.rsqrt(total_sq / width + 1e-06)[:, None]
        return (stream * factor * out_gain[None, :]).astype(BF16)

    return body


def fused_kernel(
    nz, ny, n_cb, width,
    tok, gain, gate_w, up_w, down_w, out_gain, out,
    xf, wk, dwv, asend, arecv, bsend, brecv, own, near, inv, srow, srecv, hid,
    part, keep, kgot, xsend, xgot, branch, stream, frow, fgot,
    tok_s, tok_r, sum_s, sum_r, wl, ws, wr, dl, a_s, a_r, b_s, b_r,
    hy_s, hy_r, ho_s, ho_r, hp_s, hp_r, hf_s, hf_r, k_s, k_r, x_s, x_r, g_s, g_r, f_s, f_r,
):
    n_ra = nz * ny
    tokens, depth = tok.shape
    chunks = wk.shape[0]
    half_cols = chunks * LANES
    block = tokens // nz
    half = block // 2
    subs = hid.shape[0]
    sub = block // subs
    group = nz * sub
    quarter = tokens // n_cb

    ra, cb = lax.axis_index("ra"), lax.axis_index("cb")
    z, y = ra // ny, ra % ny
    yo = 1 - y
    x, k = cb // 2, cb % 2
    up_z, down_z, far_z = lax.rem(z + 1, nz), lax.rem(z + nz - 1, nz), lax.rem(z + 2, nz)
    y_peer = (z * ny + yo, cb)
    z_peer = (up_z * ny + y, cb), (down_z * ny + y, cb)
    k_peer = (ra, x * 2 + 1 - k)
    x_peer = (ra, (1 - x) * 2 + k)

    def remote(src, dst, send, recv, device):
        return pltpu.make_async_remote_copy(
            src_ref=src, dst_ref=dst, send_sem=send, recv_sem=recv, device_id=device, device_id_type=MESH
        )

    def rows(start, size):
        return pl.ds(pl.multiple_of(start, size), size)

    barrier = pltpu.get_barrier_semaphore()
    for step in range(1, n_ra):
        pl.semaphore_signal(barrier, inc=1, device_id=(lax.rem(ra + step, n_ra), cb), device_id_type=MESH)
    for peer in (k_peer, x_peer):
        pl.semaphore_signal(barrier, inc=1, device_id=peer, device_id_type=MESH)
    pl.semaphore_wait(barrier, n_ra + 1)

    def scale(q):
        r = rows(q * quarter, quarter)
        xf[r, rows(y * depth, depth)] = (tok[r, :].astype(F32) * gain[...]).astype(BF16)

    def token_copy(step, q, device):
        mine = y if step == 0 else yo
        ref = xf.at[rows(q * quarter, quarter), rows(mine * depth, depth)]
        return remote(ref, ref, tok_s.at[step], tok_r.at[step], device)

    def token_wait(step, q):
        ref = xf.at[rows(q * quarter, quarter), rows(yo * depth, depth)]
        remote(ref, ref, tok_s.at[step], tok_r.at[step], y_peer).wait_recv()

    def w_slot(j, i):
        return wk.at[j, rows(y * depth, depth), pl.ds(i * LANES, LANES)]

    def w_part(j, i, side):
        cols = pl.ds(pl.multiple_of(side * half_cols + j * LANES, LANES), LANES)
        return (gate_w, up_w)[i].at[:, cols]

    def w_send(j, i):
        return remote(w_part(j, i, yo), w_slot(j, i), ws.at[j, i], wr.at[j, i], y_peer)

    def w_keep(j, i):
        return pltpu.make_async_copy(w_part(j, i, y), w_slot(j, i), wl.at[j, i])

    def w_wait(j):
        for i in range(2):
            dst = wk.at[j, rows(yo * depth, depth), pl.ds(i * LANES, LANES)]
            remote(dst, dst, ws.at[j, i], wr.at[j, i], y_peer).wait_recv()

    scale(cb)
    token_copy(0, cb, y_peer).start()

    @pl.loop(0, chunks)
    def _(j):
        for i in range(2):
            w_send(j, i).start()
            w_keep(j, i).start()

    down_copy = pltpu.make_async_copy(down_w, dwv, dl)
    down_copy.start()

    for step in range(1, n_cb):
        scale(lax.rem(cb + step, n_cb))

    ones = jnp.ones((8, depth), F32)

    def row_sums(value):
        return lax.dot_general(
            ones, value * value, (((1,), (1,)), ((), ())), precision=lax.Precision.HIGHEST, preferred_element_type=F32
        )

    for b in range(nz):
        srow[b] = row_sums(tok[b * block : (b + 1) * block, :].astype(F32))
    srecv[ra] = srow[z]

    def sum_copy(step):
        peer = lax.rem(ra + step, n_ra)
        return remote(srow.at[peer // ny], srecv.at[ra], sum_s.at[step], sum_r.at[step], (peer, cb))

    for step in range(1, n_ra):
        sum_copy(step).start()

    token_wait(0, cb)
    token_copy(1, cb, x_peer).start()
    token_copy(2, cb, k_peer).start()
    xq = lax.rem(cb + 2, n_cb)
    kq = x * 2 + 1 - k
    kxq = (1 - x) * 2 + 1 - k
    token_wait(1, xq)
    token_copy(3, xq, k_peer).start()

    for step in range(1, n_ra):
        src = lax.rem(ra + n_ra - step, n_ra)
        remote(srow.at[z], srecv.at[src], sum_s.at[step], sum_r.at[step], (src, cb)).wait_recv()
    total = srecv[0]
    for r in range(1, n_ra):
        total = total + srecv[r]
    scale_row = lax.rsqrt(total / width + EPS)
    inv[...] = jnp.transpose(jnp.broadcast_to(scale_row[0:1, :], (LANES, block)))

    token_wait(2, kq)
    token_wait(3, kxq)

    def a_copy(j, d):
        return remote(asend.at[j, d], arecv.at[j, d], a_s.at[j, d], a_r.at[j, d], z_peer[d])

    def b_copy(j, d):
        return remote(bsend.at[j, d], brecv.at[j, d], b_s.at[j, d], b_r.at[j, d], z_peer[d])

    def product(j, b):
        return jnp.dot(xf[rows(b * block, block), :], wk[j], preferred_element_type=F32)

    def hid_cols(side, j):
        return pl.ds(pl.multiple_of(side * half_cols + j * LANES, LANES), LANES)

    @pl.loop(0, chunks + 2)
    def _(i):
        @pl.when(i < chunks)
        def _():
            j = i
            for e in range(2):
                w_keep(j, e).wait()
            w_wait(j)
            slot = lax.rem(j, 3)
            p = product(j, far_z)
            asend[j, 0, :half, :] = p[:half].astype(BF16)
            asend[j, 1, :half, :] = p[half:].astype(BF16)
            p = product(j, up_z)
            asend[j, 0, half:, :] = p[half:].astype(BF16)
            near[slot, 0] = p[:half]
            a_copy(j, 0).start()
            p = product(j, down_z)
            asend[j, 1, half:, :] = p[:half].astype(BF16)
            near[slot, 1] = p[half:]
            a_copy(j, 1).start()
            own[slot] = product(j, z)

        @pl.when((i >= 1) & (i < chunks + 1))
        def _():
            j = i - 1
            slot = lax.rem(j, 3)
            for d in range(2):
                a_copy(j, d).wait_recv()
                bsend[j, d] = (near[slot, d] + arecv[j, d, :half, :].astype(F32)).astype(BF16)
                b_copy(j, d).start()

        @pl.when(i >= 2)
        def _():
            j = i - 2
            slot = lax.rem(j, 3)
            for d in range(2):
                b_copy(j, d).wait_recv()
            for h in range(2):
                part_rows = slice(h * half, (h + 1) * half)
                value = (
                    own[slot, part_rows, :]
                    + brecv[j, h].astype(F32)
                    + arecv[j, 1 - h, half:, :].astype(F32)
                )
                factor = inv[part_rows, :]
                gate = value[:, :LANES] * factor
                up = value[:, LANES:] * factor
                hidden = (gate / (1.0 + jnp.exp(-gate)) * up).astype(BF16)
                for s in range(subs // 2):
                    hid[h * (subs // 2) + s, rows(z * sub, sub), hid_cols(y, j)] = hidden[s * sub : (s + 1) * sub]

    def piece(s, b, side):
        return hid.at[s, rows(b * sub, sub), rows(side * half_cols, half_cols)]

    def strip(s, b, d):
        return hid.at[s, rows(b * sub + d * (sub // 2), sub // 2), :]

    def hy_copy(s):
        return remote(piece(s, z, y), piece(s, z, y), hy_s.at[s], hy_r.at[s], y_peer)

    def hy_wait(s):
        remote(piece(s, z, yo), piece(s, z, yo), hy_s.at[s], hy_r.at[s], y_peer).wait_recv()

    def ho_copy(s, d):
        return remote(piece(s, z, y), piece(s, z, y), ho_s.at[s, d], ho_r.at[s, d], z_peer[d])

    def hp_copy(s, d):
        return remote(piece(s, z, yo), piece(s, z, yo), hp_s.at[s, d], hp_r.at[s, d], z_peer[d])

    came = (down_z, up_z)

    def near_wait(s, d):
        for side, send, recv in ((y, ho_s, ho_r), (yo, hp_s, hp_r)):
            ref = piece(s, came[d], side)
            remote(ref, ref, send.at[s, d], recv.at[s, d], z_peer[d]).wait_recv()

    def hf_copy(s, d):
        ref = strip(s, came[d], d)
        return remote(ref, ref, hf_s.at[s, d], hf_r.at[s, d], z_peer[d])

    def hf_wait(s, d):
        ref = strip(s, far_z, d)
        remote(ref, ref, hf_s.at[s, d], hf_r.at[s, d], z_peer[d]).wait_recv()

    half_group = group // 2
    my_half, other_half = rows(k * half_group, half_group), rows((1 - k) * half_group, half_group)

    def k_copy(s):
        return remote(part.at[s, other_half, :], kgot.at[s], k_s.at[s], k_r.at[s], k_peer)

    def x_copy(s):
        return remote(xsend.at[s], xgot.at[s], x_s.at[s], x_r.at[s], x_peer)

    def g_copy(s):
        ref = branch.at[s, my_half, :]
        return remote(ref, ref, g_s.at[s], g_r.at[s], k_peer)

    def g_wait(s):
        ref = branch.at[s, other_half, :]
        remote(ref, ref, g_s.at[s], g_r.at[s], k_peer).wait_recv()

    def f_copy(s, step):
        peer = lax.rem(ra + step, n_ra)
        return remote(frow.at[s], fgot.at[s, ra], f_s.at[s, step], f_r.at[s, step], (peer, cb))

    def f_wait(s, step):
        src = lax.rem(ra + n_ra - step, n_ra)
        remote(frow.at[s], fgot.at[s, src], f_s.at[s, step], f_r.at[s, step], (src, cb)).wait_recv()

    def send_own(s):
        hy_copy(s).start()
        for d in range(2):
            ho_copy(s, d).start()

    send_own(0)
    down_copy.wait()

    @pl.loop(0, subs + 2)
    def _(t):
        @pl.when(t < subs)
        def _():
            hy_wait(t)
            for d in range(2):
                hp_copy(t, d).start()

        @pl.when(t + 1 < subs)
        def _():
            send_own(t + 1)

        @pl.when((t >= 1) & (t < subs + 1))
        def _():
            s = t - 1
            k_copy(s).wait_recv()
            xsend[s] = (keep[s] + kgot[s].astype(F32)).astype(BF16)
            x_copy(s).start()

        @pl.when(t < subs)
        def _():
            for d in range(2):
                near_wait(t, d)
                hf_copy(t, d).start()

        @pl.when((t >= 1) & (t < subs + 1))
        def _():
            s = t - 1
            x_copy(s).wait_recv()
            branch[s, my_half, :] = (xsend[s].astype(F32) + xgot[s].astype(F32)).astype(BF16)
            g_copy(s).start()

        @pl.when(t < subs)
        def _():
            for d in range(2):
                hf_wait(t, d)
            value = jnp.dot(hid[t], dwv[...], preferred_element_type=F32)
            part[t] = value.astype(BF16)
            stream[t] = value
            keep[t] = stream[t, my_half, :]
            k_copy(t).start()

        @pl.when((t >= 1) & (t < subs + 1))
        def _():
            s = t - 1
            g_wait(s)
            for b in range(nz):
                r = slice(b * sub, (b + 1) * sub)
                new = 0.5 * tok[rows(b * block + s * sub, sub), :].astype(F32) + branch[s, r, :].astype(F32)
                stream[s, r, :] = new
            frow[s] = row_sums(stream[s])
            fgot[s, ra] = frow[s]
            for step in range(1, n_ra):
                f_copy(s, step).start()

        @pl.when(t >= 2)
        def _():
            s = t - 2
            for step in range(1, n_ra):
                f_wait(s, step)
            total = fgot[s, 0]
            for r in range(1, n_ra):
                total = total + fgot[s, r]
            factor_row = lax.rsqrt(total / width + EPS)
            factor = jnp.transpose(jnp.broadcast_to(factor_row[0:1, :], (LANES, group)))
            for b in range(nz):
                r = slice(b * sub, (b + 1) * sub)
                to = rows(b * block + s * sub, sub)
                for c in range(depth // LANES):
                    cols = slice(c * LANES, (c + 1) * LANES)
                    out[to, cols] = (stream[s, r, cols] * factor[r, :] * out_gain[:, cols]).astype(BF16)

    for step, (q, device) in enumerate(((cb, y_peer), (cb, x_peer), (cb, k_peer), (xq, k_peer))):
        token_copy(step, q, device).wait_send()
    for step in range(1, n_ra):
        sum_copy(step).wait_send()

    @pl.loop(0, chunks)
    def _(j):
        for i in range(2):
            w_send(j, i).wait_send()
        for d in range(2):
            a_copy(j, d).wait_send()
            b_copy(j, d).wait_send()

    @pl.loop(0, subs)
    def _(s):
        hy_copy(s).wait_send()
        for d in range(2):
            ho_copy(s, d).wait_send()
            hp_copy(s, d).wait_send()
            hf_copy(s, d).wait_send()
        k_copy(s).wait_send()
        x_copy(s).wait_send()
        g_copy(s).wait_send()
        for step in range(1, n_ra):
            f_copy(s, step).wait_send()


def fused_body(nz, ny, n_cb, tokens, norm_gain, gate_weight, up_weight, down_weight, out_gain):
    n_tok, depth = tokens.shape
    n_ra = nz * ny
    units = gate_weight.shape[1]
    chunks = units // ny // LANES
    block = n_tok // nz
    subs = SUBBLOCKS
    group = n_tok // subs
    dma, vmem = pltpu.SemaphoreType.DMA, pltpu.VMEM
    scratch = [
        vmem((n_tok, ny * depth), BF16),
        vmem((chunks, ny * depth, 2 * LANES), BF16),
        vmem(down_weight.shape, BF16),
        vmem((chunks, 2, block, 2 * LANES), BF16),
        vmem((chunks, 2, block, 2 * LANES), BF16),
        vmem((chunks, 2, block // 2, 2 * LANES), BF16),
        vmem((chunks, 2, block // 2, 2 * LANES), BF16),
        vmem((3, block, 2 * LANES), F32),
        vmem((3, 2, block // 2, 2 * LANES), F32),
        vmem((block, LANES), F32),
        vmem((nz, 8, block), F32),
        vmem((n_ra, 8, block), F32),
        vmem((subs, group, units), BF16),
        vmem((subs, group, depth), BF16),
        vmem((subs, group // 2, depth), F32),
        vmem((subs, group // 2, depth), BF16),
        vmem((subs, group // 2, depth), BF16),
        vmem((subs, group // 2, depth), BF16),
        vmem((subs, group, depth), BF16),
        vmem((subs, group, depth), F32),
        vmem((subs, 8, group), F32),
        vmem((subs, n_ra, 8, group), F32),
        dma((4,)), dma((4,)), dma((n_ra,)), dma((n_ra,)),
        dma((chunks, 2)), dma((chunks, 2)), dma((chunks, 2)), dma,
        dma((chunks, 2)), dma((chunks, 2)), dma((chunks, 2)), dma((chunks, 2)),
        dma((subs,)), dma((subs,)),
        dma((subs, 2)), dma((subs, 2)), dma((subs, 2)), dma((subs, 2)), dma((subs, 2)), dma((subs, 2)),
        dma((subs,)), dma((subs,)), dma((subs,)), dma((subs,)), dma((subs,)), dma((subs,)),
        dma((subs, n_ra)), dma((subs, n_ra)),
    ]
    on_chip, anywhere = pl.BlockSpec(memory_space=vmem), pl.BlockSpec(memory_space=pl.ANY)
    return pl.pallas_call(
        functools.partial(fused_kernel, nz, ny, n_cb, depth * n_ra),
        out_shape=jax.ShapeDtypeStruct(tokens.shape, BF16),
        in_specs=[on_chip, on_chip, anywhere, anywhere, anywhere, on_chip],
        out_specs=on_chip,
        scratch_shapes=scratch,
        compiler_params=pltpu.CompilerParams(
            collective_id=0, has_side_effects=True, vmem_limit_bytes=64000 * 1024
        ),
    )(tokens, norm_gain[None, :], gate_weight, up_weight, down_weight, out_gain[None, :])


def solution(mesh):
    n_ra, n_cb = mesh.shape["ra"], mesh.shape["cb"]
    nz, ny = plane_sizes(mesh)
    plain = ring_body(mesh)

    def body(tokens, norm_gain, gate_weight, up_weight, down_weight, out_gain):
        args = (tokens, norm_gain, gate_weight, up_weight, down_weight, out_gain)
        whole = (
            nz == 4 and ny == 2 and n_cb == 4
            and gate_weight.shape[1] % (ny * LANES) == 0
            and tokens.shape[0] % (nz * SUBBLOCKS * 32) == 0
            and tokens.shape[1] % LANES == 0
        )
        return fused_body(nz, ny, n_cb, *args) if whole else plain(*args)

    placed = (P(None, "ra"), P("ra"), P("ra", "cb"), P("ra", "cb"), P("cb", "ra"), P("ra"))
    return jax.shard_map(body, mesh=mesh, in_specs=placed, out_specs=P(None, "ra"), check_vma=False)
```

```python
import functools

import jax
import jax.numpy as jnp
from jax import lax
from jax.experimental import pallas as pl
from jax.experimental.pallas import tpu as pltpu
from jax.sharding import PartitionSpec as P

F32, BF16 = jnp.float32, jnp.bfloat16
MESH = pl.DeviceIdType.MESH
LANES = 128
LANES_PER_STEP = 2 * LANES
STEPS, GROUPS, PIECES = 4, 8, 2
HOP_LAG, GATHER_LAG, DOWN_LAG = 3, 2, 12
EPS = 1e-06


def plane_sizes(mesh):
    n = mesh.shape["ra"]
    column = mesh.devices[:, 0]
    coords = [getattr(d, "coords", None) for d in column]
    if all(c is not None for c in coords):
        ny = len({c[1] for c in coords})
    else:
        ny = 2 if n % 2 == 0 else 1
    return n // ny, ny


def ring_order(mesh):
    n = mesh.shape["ra"]
    column = mesh.devices[:, 0]
    coords = [getattr(d, "coords", None) for d in column]
    if all(c is not None for c in coords):
        ny = len({c[1] for c in coords})
    else:
        ny = 2 if n % 2 == 0 else 1
    nz = n // ny
    if ny == 1 or nz % 2 or nz * ny != n:
        return list(range(n))
    walk = []
    for z in range(nz):
        ys = range(1, ny) if z % 2 == 0 else range(ny - 1, 0, -1)
        walk += [z * ny + y for y in ys]
    return walk + [z * ny for z in reversed(range(nz))]


def butterfly(value, axis, n, narrow=None):
    if n & (n - 1):
        return lax.psum(value, axis)
    step = 1
    while step < n:
        sent = value if narrow is None else value.astype(narrow)
        got = lax.ppermute(sent, axis, [(i, i ^ step) for i in range(n)])
        value = sent.astype(F32) + got.astype(F32)
        step *= 2
    return value


def ring_body(mesh):
    n_ra, n_cb = mesh.shape["ra"], mesh.shape["cb"]
    order = ring_order(mesh)
    place = [order.index(i) for i in range(n_ra)]
    to_right = [(order[i], order[(i + 1) % n_ra]) for i in range(n_ra)]
    to_left = [(order[i], order[(i - 1) % n_ra]) for i in range(n_ra)]
    far = n_ra // 2

    def body(tokens, norm_gain, gate_weight, up_weight, down_weight, out_gain):
        rows = tokens.shape[0] // n_ra
        width = tokens.shape[1] * n_ra
        hidden_cols = gate_weight.shape[1]
        cut = -(-hidden_cols // 256) * 128
        cols = (slice(0, cut), slice(cut, hidden_cols))
        p = jnp.asarray(place, jnp.int32)[lax.axis_index("ra")]

        def block(array, b):
            start = lax.rem(p + b + n_ra, n_ra) * rows
            return lax.dynamic_slice_in_dim(array, start, rows, 0)

        stream_in = tokens.astype(F32)
        scaled = (stream_in * norm_gain[None, :]).astype(BF16)
        weights = {"g": gate_weight, "u": up_weight}

        def parts(source, offsets):
            x = jnp.concatenate([block(source, b) for b in offsets], axis=0)
            return {k: jnp.dot(x, w, preferred_element_type=F32) for k, w in weights.items()}

        right, left = {}, {}
        source = scaled
        for d in range(far, 0, -1):
            mine = parts(source, (d,) if d == far else (d, -d))
            if d < far:
                source, right["g"] = lax.optimization_barrier((source, right["g"]))
            for key in ("g", "u"):
                for flow, perm, skip, at in ((right, to_right, "u", 0), (left, to_left, "g", rows)):
                    if d == far and key == skip:
                        continue
                    value = mine[key] if d == far else mine[key][at : at + rows]
                    if key in flow:
                        value = value + flow[key].astype(F32)
                    flow[key] = lax.ppermute(value.astype(BF16), "ra", perm)
        mine = parts(source, (0,))

        squares = jnp.sum(stream_in * stream_in, axis=1)
        sq = block(squares, 0)
        for k in range(1, n_ra):
            perm = [(order[i], order[(i + k) % n_ra]) for i in range(n_ra)]
            sq = sq + lax.ppermute(block(squares, k), "ra", perm)
        inv_rms = lax.rsqrt(sq / width + 1e-06)[:, None]

        total = {}
        for key in ("g", "u"):
            value = mine[key]
            for flow in (right, left):
                if key in flow:
                    value = value + flow[key].astype(F32)
            total[key] = value * inv_rms
        own = (jax.nn.silu(total["g"]) * total["u"]).astype(BF16)

        stream = jnp.zeros(tokens.shape, F32)
        sums = jnp.zeros(tokens.shape[:1], F32)

        def finish(stream, sums, held):
            units = jnp.concatenate([h for _, h in held], axis=0)
            down = jnp.dot(units, down_weight, preferred_element_type=F32)
            branch = butterfly(down, "cb", n_cb, BF16)
            for i, (b, _) in enumerate(held):
                new = 0.5 * block(stream_in, b) + branch[i * rows : (i + 1) * rows]
                start = lax.rem(p + b + n_ra, n_ra) * rows
                stream = lax.dynamic_update_slice_in_dim(stream, new, start, 0)
                sums = lax.dynamic_update_slice_in_dim(sums, jnp.sum(new * new, axis=1), start, 0)
            return stream, sums

        from_left = from_right = own
        pending = [(0, own)]
        for s in range(1, far + 1):
            last = s == far
            if last:
                from_left, from_right = from_left[:, cols[0]], from_right[:, cols[1]]
            from_left = lax.ppermute(from_left, "ra", to_right)
            from_right = lax.ppermute(from_right, "ra", to_left)
            stream, sums = finish(stream, sums, pending)
            if last:
                pending = [(far, jnp.concatenate([from_left, from_right], axis=1))]
            else:
                pending = [(-s, from_left), (s, from_right)]
        stream, sums = finish(stream, sums, pending)

        total_sq = butterfly(sums, "ra", n_ra)
        factor = lax.rsqrt(total_sq / width + 1e-06)[:, None]
        return (stream * factor * out_gain[None, :]).astype(BF16)

    return body


def fused_kernel(
    nz, ny, n_cb, width,
    tok, gain, gate_w, up_w, down_w, out_gain, out,
    xf, wk, dwv, pbuf, rsend, rrecv, inv, srow, speer, csend, crecv, hid,
    part, keep, kgot, yown, ysend, ygot, xsend, xgot, branch, stream, frow, fgot,
    tok_s, tok_r, sum_s, sum_r, c_s, c_r, wl, ws, wr, dl, ds, dr, r_s, r_r, h_s, h_r,
    k_s, k_r, y_s, y_r, x_s, x_r, g_s, g_r, f_s, f_r,
):
    n_ra = nz * ny
    tokens, depth = tok.shape
    chunks = wk.shape[0]
    half_cols = chunks * LANES
    half = tokens // 2
    step_rows = half // STEPS
    quarter = tokens // n_cb
    piece_rows = quarter // PIECES
    block = tokens // nz
    messages = chunks * STEPS
    groups, group, _ = hid.shape
    side_rows = group // 2
    batches = frow.shape[0]
    per_batch = groups // batches
    gather_parts = 2
    gather_rows = side_rows // gather_parts
    gathers = groups * gather_parts

    ra, cb = lax.axis_index("ra"), lax.axis_index("cb")
    z, y = ra // ny, ra % ny
    yo = 1 - y
    x, k = cb // 2, cb % 2
    last = nz - 1
    y_peer = (z * ny + yo, cb)
    z_peer = (lax.rem(z + 1, nz) * ny + y, cb), (lax.rem(z + last, nz) * ny + y, cb)
    k_peer = (ra, x * 2 + 1 - k)
    x_peer = (ra, (1 - x) * 2 + k)
    place = (z, last - z)

    def remote(src, dst, send, recv, device):
        return pltpu.make_async_remote_copy(
            src_ref=src, dst_ref=dst, send_sem=send, recv_sem=recv, device_id=device, device_id_type=MESH
        )

    def rows(start, size):
        return pl.ds(pl.multiple_of(start, size), size)

    barrier = pltpu.get_barrier_semaphore()
    for peer in (y_peer, k_peer, x_peer):
        pl.semaphore_signal(barrier, inc=1, device_id=peer, device_id_type=MESH)
    for d in range(2):
        @pl.when(place[d] < last)
        def _():
            pl.semaphore_signal(barrier, inc=1, device_id=z_peer[d], device_id_type=MESH)
    pl.semaphore_wait(barrier, 3 + jnp.minimum(z, 1) + jnp.minimum(last - z, 1))

    def token_ref(q, p, side):
        return xf.at[rows(q * quarter + p * piece_rows, piece_rows), rows(side * depth, depth)]

    def scale(q, p):
        r = rows(q * quarter + p * piece_rows, piece_rows)
        xf[r, rows(y * depth, depth)] = (tok[r, :].astype(F32) * gain[...]).astype(BF16)

    xq = lax.rem(cb + 2, n_cb)
    kq = x * 2 + 1 - k
    kxq = (1 - x) * 2 + 1 - k
    token_moves = ((cb, y, y_peer), (cb, yo, x_peer), (cb, yo, k_peer), (xq, yo, k_peer))

    def token_copy(kind, p):
        q, side, device = token_moves[kind]
        return remote(token_ref(q, p, side), token_ref(q, p, side), tok_s.at[kind, p], tok_r.at[kind, p], device)

    def token_wait(kind, p):
        ref = token_ref((cb, xq, kq, kxq)[kind], p, yo)
        remote(ref, ref, tok_s.at[kind, p], tok_r.at[kind, p], y_peer).wait_recv()

    def w_slot(j, i):
        return wk.at[j, rows(y * depth, depth), pl.ds(i * LANES, LANES)]

    def w_part(j, i, side):
        cols = pl.ds(pl.multiple_of(side * half_cols + j * LANES, LANES), LANES)
        return (gate_w, up_w)[i].at[:, cols]

    def w_send(j, i):
        return remote(w_part(j, i, yo), w_slot(j, i), ws.at[j, i], wr.at[j, i], y_peer)

    def w_keep(j, i):
        return pltpu.make_async_copy(w_part(j, i, y), w_slot(j, i), wl.at[j, i])

    def w_wait(j, i):
        dst = wk.at[j, rows(yo * depth, depth), pl.ds(i * LANES, LANES)]
        remote(dst, dst, ws.at[j, i], wr.at[j, i], y_peer).wait_recv()

    def down_rows(side):
        return down_w.at[rows(side * half_cols, half_cols), :]

    down_here = dwv.at[:, rows(y * depth, depth)]
    down_there = dwv.at[:, rows(yo * depth, depth)]

    def down_send():
        return remote(down_rows(yo), down_here, ds, dr, y_peer)

    def down_wait():
        remote(down_there, down_there, ds, dr, y_peer).wait_recv()

    def down_keep():
        return pltpu.make_async_copy(down_rows(y), down_here, dl)

    def row_sums(value):
        square = value * value
        folded = square[:, :LANES]
        for c in range(1, depth // LANES):
            folded = folded + square[:, c * LANES : (c + 1) * LANES]
        total = jnp.sum(jnp.transpose(folded), axis=0, keepdims=True)
        return jnp.broadcast_to(total, (8, value.shape[0]))

    def inverse(total, count):
        row = lax.rsqrt(total / width + EPS)
        return jnp.transpose(jnp.broadcast_to(row[0:1, :], (LANES, count)))

    def sum_copy():
        return remote(srow, speer, sum_s, sum_r, y_peer)

    with jax.named_scope("scale"):
        for p in range(PIECES):
            scale(cb, p)
            token_copy(0, p).start()
        for step in range(1, n_cb):
            for p in range(PIECES):
                scale(lax.rem(cb + step, n_cb), p)
    with jax.named_scope("sums"):
        for b in range(nz):
            r = slice(b * block, (b + 1) * block)
            srow[:, r] = row_sums(tok[r, :].astype(F32))
        sum_copy().start()

    with jax.named_scope("issue"):
        @pl.loop(0, chunks)
        def _(j):
            for i in range(2):
                w_send(j, i).start()
            for i in range(2):
                w_keep(j, i).start()

        down_send().start()
        down_keep().start()

    with jax.named_scope("tokens_y"):
        for p in range(PIECES):
            token_wait(0, p)
            token_copy(1, p).start()
            token_copy(2, p).start()
    with jax.named_scope("tokens_x"):
        for p in range(PIECES):
            token_wait(1, p)
            token_copy(3, p).start()
        for p in range(PIECES):
            token_wait(2, p)
            token_wait(3, p)
    with jax.named_scope("sums_y"):
        sum_copy().wait()
        srow[...] = srow[...] + speer[...]

    def r_copy(d, m):
        return remote(rsend.at[d, m], rrecv.at[d, m], r_s.at[d, m], r_r.at[d, m], z_peer[d])

    def c_copy(d):
        return remote(csend.at[d], crecv.at[d], c_s.at[d], c_r.at[d], z_peer[d])

    def hidden_block(d, j, q, value):
        factor = inv[rows(q * step_rows, step_rows), :]
        gate = value[:, :LANES] * factor
        up = value[:, LANES:] * factor
        hidden = (gate / (1.0 + jnp.exp(-gate)) * up).astype(BF16)
        per = step_rows // side_rows
        for s in range(per):
            cols = rows(j * LANES, LANES)
            hid[q * per + s, pl.ds((1 - d) * side_rows, side_rows), cols] = hidden[s * side_rows : (s + 1) * side_rows]

    def reduce_step(d, i):
        at = place[d]
        m = i - HOP_LAG * at
        start = (1 - d) * half

        @pl.when((m >= 0) & (m < messages))
        def _():
            j, q = m // STEPS, lax.rem(m, STEPS)
            slot = lax.rem(j, 4)
            r = rows(start + q * step_rows, step_rows)
            sums = slice(start, start + half)

            @pl.when(at == 0)
            def _():
                @pl.when(m == 0)
                def _():
                    csend[d] = srow[:, sums]
                    c_copy(d).start()

                rsend[d, m] = pbuf[slot, r, :].astype(BF16)
                r_copy(d, m).start()

            @pl.when((at > 0) & (at < last))
            def _():
                @pl.when(m == 0)
                def _():
                    c_copy(d).wait_recv()
                    csend[d] = srow[:, sums] + crecv[d]
                    c_copy(d).start()

                r_copy(d, m).wait_recv()
                rsend[d, m] = (pbuf[slot, r, :] + rrecv[d, m].astype(F32)).astype(BF16)
                r_copy(d, m).start()

            @pl.when(at == last)
            def _():
                @pl.when(m == 0)
                def _():
                    c_copy(d).wait_recv()
                    inv[...] = inverse(srow[:, sums] + crecv[d], half)

                r_copy(d, m).wait_recv()
                hidden_block(d, j, q, pbuf[slot, r, :] + rrecv[d, m].astype(F32))

    @pl.loop(0, messages + HOP_LAG * last)
    def _(i):
        @pl.when((lax.rem(i, STEPS) == 0) & (i < messages))
        def _():
            with jax.named_scope("product"):
                j = i // STEPS
                for e in range(2):
                    w_keep(j, e).wait()
                    w_wait(j, e)
                for b in range(nz):
                    r = slice(b * block, (b + 1) * block)
                    pbuf[lax.rem(j, 4), r, :] = jnp.dot(xf[r, :], wk[j], preferred_element_type=F32)

        with jax.named_scope("reduce"):
            for d in range(2):
                reduce_step(d, i)

    def gather_ref(d, u):
        part = lax.rem(u, gather_parts)
        return hid.at[u // gather_parts, rows(d * side_rows + part * gather_rows, gather_rows), :]

    def h_copy(d, u):
        return remote(gather_ref(d, u), gather_ref(d, u), h_s.at[d, u], h_r.at[d, u], z_peer[d])

    def gather_step(d, i):
        at = place[d]
        u = i - GATHER_LAG * at

        @pl.when((u >= 0) & (u < gathers))
        def _():
            @pl.when(at > 0)
            def _():
                h_copy(d, u).wait_recv()

            @pl.when(at < last)
            def _():
                h_copy(d, u).start()

    mine, other = rows(k * side_rows, side_rows), rows((1 - k) * side_rows, side_rows)
    cols_here, cols_there = rows(y * depth, depth), rows(yo * depth, depth)

    def k_copy(g):
        return remote(part.at[g, other, :], kgot.at[g], k_s.at[g], k_r.at[g], k_peer)

    def y_copy(g):
        return remote(ysend.at[g], ygot.at[g], y_s.at[g], y_r.at[g], y_peer)

    def x_copy(g):
        return remote(xsend.at[g], xgot.at[g], x_s.at[g], x_r.at[g], x_peer)

    def g_copy(g):
        ref = branch.at[g, mine, :]
        return remote(ref, ref, g_s.at[g], g_r.at[g], k_peer)

    def g_wait(g):
        ref = branch.at[g, other, :]
        remote(ref, ref, g_s.at[g], g_r.at[g], k_peer).wait_recv()

    def f_copy(b, step):
        peer = lax.rem(ra + step, n_ra)
        return remote(frow.at[b], fgot.at[b, ra], f_s.at[b, step], f_r.at[b, step], (peer, cb))

    def f_wait(b, step):
        src = lax.rem(ra + n_ra - step, n_ra)
        remote(frow.at[b], fgot.at[b, src], f_s.at[b, step], f_r.at[b, step], (src, cb)).wait_recv()

    def down_product(g):
        value = jnp.dot(hid[g], dwv[...], preferred_element_type=F32)
        part[g] = value.astype(BF16)
        keep[...] = value
        yown[g] = keep[mine, :]
        k_copy(g).start()

    def core_sum(g):
        k_copy(g).wait_recv()
        ysend[g] = (yown[g, :, cols_there] + kgot[g, :, cols_there].astype(F32)).astype(BF16)
        y_copy(g).start()

    def y_sum(g):
        y_copy(g).wait_recv()
        value = yown[g, :, cols_here] + kgot[g, :, cols_here].astype(F32) + ygot[g].astype(F32)
        xsend[g] = value.astype(BF16)
        x_copy(g).start()

    def x_sum(g):
        x_copy(g).wait_recv()
        branch[g, mine, :] = (xsend[g].astype(F32) + xgot[g].astype(F32)).astype(BF16)
        g_copy(g).start()

    def new_stream(g):
        g_wait(g)
        for side in range(2):
            r = slice(side * side_rows, (side + 1) * side_rows)
            old = tok[rows(side * half + g * side_rows, side_rows), :].astype(F32)
            stream[g, r, :] = 0.5 * old + branch[g, r, :].astype(F32)
        b, place_in = g // per_batch, lax.rem(g, per_batch)
        frow[b, :, rows(place_in * group, group)] = row_sums(stream[g])

        @pl.when(place_in == per_batch - 1)
        def _():
            fgot[b, ra] = frow[b]
            for step in range(1, n_ra):
                f_copy(b, step).start()

    def finish(b):
        for step in range(1, n_ra):
            f_wait(b, step)
        total = fgot[b, 0]
        for r in range(1, n_ra):
            total = total + fgot[b, r]
        factor = inverse(total, per_batch * group)
        for e in range(per_batch):
            g = b * per_batch + e
            for side in range(2):
                r = slice(side * side_rows, (side + 1) * side_rows)
                f = factor[e * group + side * side_rows : e * group + (side + 1) * side_rows, :]
                to = rows(side * half + g * side_rows, side_rows)
                for c in range(depth // LANES):
                    cols = slice(c * LANES, (c + 1) * LANES)
                    out[to, cols] = (stream[g, r, cols] * f * out_gain[:, cols]).astype(BF16)

    stages = (core_sum, y_sum, x_sum, new_stream)
    names = ("core_sum", "y_sum", "x_sum", "new_stream")
    turns = groups + len(stages)

    @pl.loop(0, DOWN_LAG + gather_parts * turns)
    def _(i):
        with jax.named_scope("gather"):
            for d in range(2):
                gather_step(d, i)

        behind = i - DOWN_LAG
        t = behind // gather_parts

        @pl.when((behind >= 0) & (lax.rem(behind, gather_parts) == 0))
        def _():
            @pl.when(t == 0)
            def _():
                with jax.named_scope("down_wait"):
                    down_keep().wait()
                    down_wait()

            for n, stage in reversed(list(enumerate(stages, 1))):
                @pl.when((t >= n) & (t < groups + n))
                def _():
                    with jax.named_scope(names[n - 1]):
                        stage(t - n)

            @pl.when(t < groups)
            def _():
                with jax.named_scope("down"):
                    down_product(t)

            for b in range(batches - 1):
                @pl.when(t == (b + 1) * per_batch + len(stages) + 1)
                def _():
                    with jax.named_scope("finish"):
                        finish(b)

    with jax.named_scope("finish"):
        finish(batches - 1)

    with jax.named_scope("drain"):
        for kind in range(len(token_moves)):
            for p in range(PIECES):
                token_copy(kind, p).wait_send()
        down_send().wait_send()

        @pl.loop(0, chunks)
        def _(j):
            for i in range(2):
                w_send(j, i).wait_send()

        for d in range(2):
            @pl.when(place[d] < last)
            def _():
                c_copy(d).wait_send()

                @pl.loop(0, messages)
                def _(m):
                    r_copy(d, m).wait_send()

                @pl.loop(0, gathers)
                def _(u):
                    h_copy(d, u).wait_send()

        @pl.loop(0, groups)
        def _(g):
            for copy in (k_copy, y_copy, x_copy, g_copy):
                copy(g).wait_send()

        for b in range(batches):
            for step in range(1, n_ra):
                f_copy(b, step).wait_send()


def fused_body(nz, ny, n_cb, tokens, norm_gain, gate_weight, up_weight, down_weight, out_gain):
    n_tok, depth = tokens.shape
    n_ra = nz * ny
    units = gate_weight.shape[1] // ny
    chunks = units // LANES
    half = n_tok // 2
    messages = chunks * STEPS
    group = n_tok // GROUPS
    side = group // 2
    batches = 2
    dma, vmem = pltpu.SemaphoreType.DMA, pltpu.VMEM
    scratch = [
        vmem((n_tok, ny * depth), BF16),
        vmem((chunks, ny * depth, LANES_PER_STEP), BF16),
        vmem((units, ny * depth), BF16),
        vmem((4, n_tok, LANES_PER_STEP), F32),
        vmem((2, messages, half // STEPS, LANES_PER_STEP), BF16),
        vmem((2, messages, half // STEPS, LANES_PER_STEP), BF16),
        vmem((half, LANES), F32),
        vmem((8, n_tok), F32),
        vmem((8, n_tok), F32),
        vmem((2, 8, half), F32),
        vmem((2, 8, half), F32),
        vmem((GROUPS, group, units), BF16),
        vmem((GROUPS, group, ny * depth), BF16),
        vmem((group, ny * depth), F32),
        vmem((GROUPS, side, ny * depth), BF16),
        vmem((GROUPS, side, ny * depth), F32),
        vmem((GROUPS, side, depth), BF16),
        vmem((GROUPS, side, depth), BF16),
        vmem((GROUPS, side, depth), BF16),
        vmem((GROUPS, side, depth), BF16),
        vmem((GROUPS, group, depth), BF16),
        vmem((GROUPS, group, depth), F32),
        vmem((batches, 8, n_tok // batches), F32),
        vmem((batches, n_ra, 8, n_tok // batches), F32),
        dma((4, PIECES)), dma((4, PIECES)), dma, dma, dma((2,)), dma((2,)),
        dma((chunks, 2)), dma((chunks, 2)), dma((chunks, 2)), dma, dma, dma,
        dma((2, messages)), dma((2, messages)), dma((2, GROUPS * 2)), dma((2, GROUPS * 2)),
        dma((GROUPS,)), dma((GROUPS,)), dma((GROUPS,)), dma((GROUPS,)),
        dma((GROUPS,)), dma((GROUPS,)), dma((GROUPS,)), dma((GROUPS,)),
        dma((batches, n_ra)), dma((batches, n_ra)),
    ]
    on_chip, anywhere = pl.BlockSpec(memory_space=vmem), pl.BlockSpec(memory_space=pl.ANY)
    return pl.pallas_call(
        functools.partial(fused_kernel, nz, ny, n_cb, depth * n_ra),
        out_shape=jax.ShapeDtypeStruct(tokens.shape, BF16),
        in_specs=[on_chip, on_chip, anywhere, anywhere, anywhere, on_chip],
        out_specs=on_chip,
        scratch_shapes=scratch,
        compiler_params=pltpu.CompilerParams(
            collective_id=0, has_side_effects=True, vmem_limit_bytes=64000 * 1024
        ),
    )(tokens, norm_gain[None, :], gate_weight, up_weight, down_weight, out_gain[None, :])


def solution(mesh):
    n_ra, n_cb = mesh.shape["ra"], mesh.shape["cb"]
    nz, ny = plane_sizes(mesh)
    plain = ring_body(mesh)

    def body(tokens, norm_gain, gate_weight, up_weight, down_weight, out_gain):
        args = (tokens, norm_gain, gate_weight, up_weight, down_weight, out_gain)
        whole = (
            nz == 4 and ny == 2 and n_cb == 4
            and gate_weight.shape[1] % (ny * LANES) == 0
            and tokens.shape[0] % (GROUPS * 4 * 16) == 0
            and tokens.shape[1] % LANES == 0
        )
        return fused_body(nz, ny, n_cb, *args) if whole else plain(*args)

    placed = (P(None, "ra"), P("ra"), P("ra", "cb"), P("ra", "cb"), P("cb", "ra"), P("ra"))
    return jax.shard_map(body, mesh=mesh, in_specs=placed, out_specs=P(None, "ra"), check_vma=False)
```

```python
import functools

import jax
import jax.numpy as jnp
from jax import lax
from jax.experimental import pallas as pl
from jax.experimental.pallas import tpu as pltpu
from jax.sharding import PartitionSpec as P

F32, BF16 = jnp.float32, jnp.bfloat16
MESH = pl.DeviceIdType.MESH
LANES = 128
LANES_PER_STEP = 2 * LANES
STEPS, GROUPS, PIECES = 4, 8, 2
EARLY_CHUNKS, HOP_LAG, DOWN_LAG = 3, 3, 1
STAGE_TURNS = (1, 3, 5, 6)
EPS = 1e-06


def plane_sizes(mesh):
    n = mesh.shape["ra"]
    column = mesh.devices[:, 0]
    coords = [getattr(d, "coords", None) for d in column]
    if all(c is not None for c in coords):
        ny = len({c[1] for c in coords})
    else:
        ny = 2 if n % 2 == 0 else 1
    return n // ny, ny


def ring_order(mesh):
    n = mesh.shape["ra"]
    column = mesh.devices[:, 0]
    coords = [getattr(d, "coords", None) for d in column]
    if all(c is not None for c in coords):
        ny = len({c[1] for c in coords})
    else:
        ny = 2 if n % 2 == 0 else 1
    nz = n // ny
    if ny == 1 or nz % 2 or nz * ny != n:
        return list(range(n))
    walk = []
    for z in range(nz):
        ys = range(1, ny) if z % 2 == 0 else range(ny - 1, 0, -1)
        walk += [z * ny + y for y in ys]
    return walk + [z * ny for z in reversed(range(nz))]


def butterfly(value, axis, n, narrow=None):
    if n & (n - 1):
        return lax.psum(value, axis)
    step = 1
    while step < n:
        sent = value if narrow is None else value.astype(narrow)
        got = lax.ppermute(sent, axis, [(i, i ^ step) for i in range(n)])
        value = sent.astype(F32) + got.astype(F32)
        step *= 2
    return value


def ring_body(mesh):
    n_ra, n_cb = mesh.shape["ra"], mesh.shape["cb"]
    order = ring_order(mesh)
    place = [order.index(i) for i in range(n_ra)]
    to_right = [(order[i], order[(i + 1) % n_ra]) for i in range(n_ra)]
    to_left = [(order[i], order[(i - 1) % n_ra]) for i in range(n_ra)]
    far = n_ra // 2

    def body(tokens, norm_gain, gate_weight, up_weight, down_weight, out_gain):
        rows = tokens.shape[0] // n_ra
        width = tokens.shape[1] * n_ra
        hidden_cols = gate_weight.shape[1]
        cut = -(-hidden_cols // 256) * 128
        cols = (slice(0, cut), slice(cut, hidden_cols))
        p = jnp.asarray(place, jnp.int32)[lax.axis_index("ra")]

        def block(array, b):
            start = lax.rem(p + b + n_ra, n_ra) * rows
            return lax.dynamic_slice_in_dim(array, start, rows, 0)

        stream_in = tokens.astype(F32)
        scaled = (stream_in * norm_gain[None, :]).astype(BF16)
        weights = {"g": gate_weight, "u": up_weight}

        def parts(source, offsets):
            x = jnp.concatenate([block(source, b) for b in offsets], axis=0)
            return {k: jnp.dot(x, w, preferred_element_type=F32) for k, w in weights.items()}

        right, left = {}, {}
        source = scaled
        for d in range(far, 0, -1):
            mine = parts(source, (d,) if d == far else (d, -d))
            if d < far:
                source, right["g"] = lax.optimization_barrier((source, right["g"]))
            for key in ("g", "u"):
                for flow, perm, skip, at in ((right, to_right, "u", 0), (left, to_left, "g", rows)):
                    if d == far and key == skip:
                        continue
                    value = mine[key] if d == far else mine[key][at : at + rows]
                    if key in flow:
                        value = value + flow[key].astype(F32)
                    flow[key] = lax.ppermute(value.astype(BF16), "ra", perm)
        mine = parts(source, (0,))

        squares = jnp.sum(stream_in * stream_in, axis=1)
        sq = block(squares, 0)
        for k in range(1, n_ra):
            perm = [(order[i], order[(i + k) % n_ra]) for i in range(n_ra)]
            sq = sq + lax.ppermute(block(squares, k), "ra", perm)
        inv_rms = lax.rsqrt(sq / width + 1e-06)[:, None]

        total = {}
        for key in ("g", "u"):
            value = mine[key]
            for flow in (right, left):
                if key in flow:
                    value = value + flow[key].astype(F32)
            total[key] = value * inv_rms
        own = (jax.nn.silu(total["g"]) * total["u"]).astype(BF16)

        stream = jnp.zeros(tokens.shape, F32)
        sums = jnp.zeros(tokens.shape[:1], F32)

        def finish(stream, sums, held):
            units = jnp.concatenate([h for _, h in held], axis=0)
            down = jnp.dot(units, down_weight, preferred_element_type=F32)
            branch = butterfly(down, "cb", n_cb, BF16)
            for i, (b, _) in enumerate(held):
                new = 0.5 * block(stream_in, b) + branch[i * rows : (i + 1) * rows]
                start = lax.rem(p + b + n_ra, n_ra) * rows
                stream = lax.dynamic_update_slice_in_dim(stream, new, start, 0)
                sums = lax.dynamic_update_slice_in_dim(sums, jnp.sum(new * new, axis=1), start, 0)
            return stream, sums

        from_left = from_right = own
        pending = [(0, own)]
        for s in range(1, far + 1):
            last = s == far
            if last:
                from_left, from_right = from_left[:, cols[0]], from_right[:, cols[1]]
            from_left = lax.ppermute(from_left, "ra", to_right)
            from_right = lax.ppermute(from_right, "ra", to_left)
            stream, sums = finish(stream, sums, pending)
            if last:
                pending = [(far, jnp.concatenate([from_left, from_right], axis=1))]
            else:
                pending = [(-s, from_left), (s, from_right)]
        stream, sums = finish(stream, sums, pending)

        total_sq = butterfly(sums, "ra", n_ra)
        factor = lax.rsqrt(total_sq / width + 1e-06)[:, None]
        return (stream * factor * out_gain[None, :]).astype(BF16)

    return body


def fused_kernel(
    nz, ny, n_cb, width,
    tok, gain, gate_w, up_w, down_w, out_gain, out,
    xf, wk, dwv, pbuf, rsend, rrecv, inv, srow, speer, csend, crecv, hid,
    part, keep, kgot, yown, ysend, ygot, xsend, xgot, branch, stream, frow, fgot,
    tok_s, tok_r, sum_s, sum_r, c_s, c_r, wl, ws, wr, dl, ds, dr, r_s, r_r, h_s, h_r,
    k_s, k_r, y_s, y_r, x_s, x_r, g_s, g_r, f_s, f_r,
):
    n_ra = nz * ny
    tokens, depth = tok.shape
    chunks = wk.shape[0]
    half_cols = chunks * LANES
    half = tokens // 2
    step_rows = half // STEPS
    quarter = tokens // n_cb
    piece_rows = quarter // PIECES
    block = tokens // nz
    messages = chunks * STEPS
    groups, group, _ = hid.shape
    side_rows = group // 2
    batches = frow.shape[0]
    per_batch = groups // batches
    early = min(EARLY_CHUNKS, chunks - 1)
    gathers = 2 * (early + groups)

    ra, cb = lax.axis_index("ra"), lax.axis_index("cb")
    z, y = ra // ny, ra % ny
    yo = 1 - y
    x, k = cb // 2, cb % 2
    last = nz - 1
    y_peer = (z * ny + yo, cb)
    z_peer = (lax.rem(z + 1, nz) * ny + y, cb), (lax.rem(z + last, nz) * ny + y, cb)
    k_peer = (ra, x * 2 + 1 - k)
    x_peer = (ra, (1 - x) * 2 + k)
    place = (z, last - z)

    def remote(src, dst, send, recv, device):
        return pltpu.make_async_remote_copy(
            src_ref=src, dst_ref=dst, send_sem=send, recv_sem=recv, device_id=device, device_id_type=MESH
        )

    def rows(start, size):
        return pl.ds(pl.multiple_of(start, size), size)

    barrier = pltpu.get_barrier_semaphore()
    for peer in (y_peer, k_peer, x_peer):
        pl.semaphore_signal(barrier, inc=1, device_id=peer, device_id_type=MESH)
    for d in range(2):
        @pl.when(place[d] < last)
        def _():
            pl.semaphore_signal(barrier, inc=1, device_id=z_peer[d], device_id_type=MESH)
    pl.semaphore_wait(barrier, 3 + jnp.minimum(z, 1) + jnp.minimum(last - z, 1))

    def token_ref(q, p, side):
        return xf.at[rows(q * quarter + p * piece_rows, piece_rows), rows(side * depth, depth)]

    def scale(q, p):
        r = rows(q * quarter + p * piece_rows, piece_rows)
        xf[r, rows(y * depth, depth)] = (tok[r, :].astype(F32) * gain[...]).astype(BF16)

    xq = lax.rem(cb + 2, n_cb)
    kq = x * 2 + 1 - k
    kxq = (1 - x) * 2 + 1 - k
    token_moves = ((cb, y, y_peer), (cb, yo, x_peer), (cb, yo, k_peer), (xq, yo, k_peer))

    def token_copy(kind, p):
        q, side, device = token_moves[kind]
        return remote(token_ref(q, p, side), token_ref(q, p, side), tok_s.at[kind, p], tok_r.at[kind, p], device)

    def token_wait(kind, p):
        ref = token_ref((cb, xq, kq, kxq)[kind], p, yo)
        remote(ref, ref, tok_s.at[kind, p], tok_r.at[kind, p], y_peer).wait_recv()

    def w_slot(j, i):
        return wk.at[j, rows(y * depth, depth), pl.ds(i * LANES, LANES)]

    def w_part(j, i, side):
        cols = pl.ds(pl.multiple_of(side * half_cols + j * LANES, LANES), LANES)
        return (gate_w, up_w)[i].at[:, cols]

    def w_send(j, i):
        return remote(w_part(j, i, yo), w_slot(j, i), ws.at[j, i], wr.at[j, i], y_peer)

    def w_keep(j, i):
        return pltpu.make_async_copy(w_part(j, i, y), w_slot(j, i), wl.at[j, i])

    def w_wait(j, i):
        dst = wk.at[j, rows(yo * depth, depth), pl.ds(i * LANES, LANES)]
        remote(dst, dst, ws.at[j, i], wr.at[j, i], y_peer).wait_recv()

    def down_rows(side):
        return down_w.at[rows(side * half_cols, half_cols), :]

    down_here = dwv.at[:, rows(y * depth, depth)]
    down_there = dwv.at[:, rows(yo * depth, depth)]

    def down_send():
        return remote(down_rows(yo), down_here, ds, dr, y_peer)

    def down_wait():
        remote(down_there, down_there, ds, dr, y_peer).wait_recv()

    def down_keep():
        return pltpu.make_async_copy(down_rows(y), down_here, dl)

    def row_sums(value):
        square = value * value
        folded = square[:, :LANES]
        for c in range(1, depth // LANES):
            folded = folded + square[:, c * LANES : (c + 1) * LANES]
        return jnp.sum(jnp.transpose(folded), axis=0, keepdims=True)

    def spread(row):
        return jnp.transpose(jnp.broadcast_to(lax.rsqrt(row / width + EPS), (LANES, LANES)))

    def sum_copy():
        return remote(srow, speer, sum_s, sum_r, y_peer)

    with jax.named_scope("scale"):
        for p in range(PIECES):
            scale(cb, p)
            token_copy(0, p).start()
        for step in range(1, n_cb):
            for p in range(PIECES):
                scale(lax.rem(cb + step, n_cb), p)
    with jax.named_scope("sums"):
        for b in range(tokens // LANES):
            srow[b : b + 1, :] = row_sums(tok[b * LANES : (b + 1) * LANES, :].astype(F32))
        sum_copy().start()

    frow[...] = jnp.zeros_like(frow)

    with jax.named_scope("issue"):
        @pl.loop(0, chunks)
        def _(j):
            for i in range(2):
                w_send(j, i).start()
            for i in range(2):
                w_keep(j, i).start()

        down_send().start()
        down_keep().start()

    with jax.named_scope("tokens_y"):
        for p in range(PIECES):
            token_wait(0, p)
            token_copy(1, p).start()
            token_copy(2, p).start()
    with jax.named_scope("tokens_x"):
        for p in range(PIECES):
            token_wait(1, p)
            token_copy(3, p).start()
        for p in range(PIECES):
            token_wait(2, p)
            token_wait(3, p)
    with jax.named_scope("sums_y"):
        sum_copy().wait()
        srow[...] = srow[...] + speer[...]

    def r_copy(d, m):
        return remote(rsend.at[d, m], rrecv.at[d, m], r_s.at[d, m], r_r.at[d, m], z_peer[d])

    def c_copy(d):
        return remote(csend.at[d], crecv.at[d], c_s.at[d], c_r.at[d], z_peer[d])

    def hidden_block(d, j, q, value):
        factor = inv[rows(q * step_rows, step_rows), :]
        gate = value[:, :LANES] * factor
        up = value[:, LANES:] * factor
        hidden = (gate / (1.0 + jnp.exp(-gate)) * up).astype(BF16)
        per = step_rows // side_rows
        for s in range(per):
            cols = rows(j * LANES, LANES)
            hid[q * per + s, pl.ds((1 - d) * side_rows, side_rows), cols] = hidden[s * side_rows : (s + 1) * side_rows]

    def reduce_step(d, i):
        at = place[d]
        m = i - HOP_LAG * at
        start = (1 - d) * half

        @pl.when((m >= 0) & (m < messages))
        def _():
            j, q = m // STEPS, lax.rem(m, STEPS)
            slot = lax.rem(j, 4)
            r = rows(start + q * step_rows, step_rows)

            @pl.when(at == 0)
            def _():
                @pl.when(m == 0)
                def _():
                    csend[d] = srow[...]
                    c_copy(d).start()

                rsend[d, m] = pbuf[slot, r, :].astype(BF16)
                r_copy(d, m).start()

            @pl.when((at > 0) & (at < last))
            def _():
                @pl.when(m == 0)
                def _():
                    c_copy(d).wait_recv()
                    csend[d] = srow[...] + crecv[d]
                    c_copy(d).start()

                r_copy(d, m).wait_recv()
                rsend[d, m] = (pbuf[slot, r, :] + rrecv[d, m].astype(F32)).astype(BF16)
                r_copy(d, m).start()

            @pl.when(at == last)
            def _():
                @pl.when(m == 0)
                def _():
                    c_copy(d).wait_recv()
                    total = srow[...] + crecv[d]
                    for b in range(half // LANES):
                        row = start // LANES + b
                        inv[b * LANES : (b + 1) * LANES, :] = spread(total[row : row + 1, :])

                r_copy(d, m).wait_recv()
                hidden_block(d, j, q, pbuf[slot, r, :] + rrecv[d, m].astype(F32))

    def early_copy(d, v):
        lower = groups // 2
        ref = hid.at[rows(lax.rem(v, 2) * lower, lower), pl.ds(d * side_rows, side_rows), rows(v // 2 * LANES, LANES)]
        return remote(ref, ref, h_s.at[d, v], h_r.at[d, v], z_peer[d])

    def late_copy(d, v):
        u = v - 2 * early
        lower = side_rows // 2
        r = rows(d * side_rows + lax.rem(u, 2) * lower, lower)
        ref = hid.at[u // 2, r, pl.ds(early * LANES, (chunks - early) * LANES)]
        return remote(ref, ref, h_s.at[d, v], h_r.at[d, v], z_peer[d])

    def pass_on(copy, at):
        @pl.when(at > 0)
        def _():
            copy.wait_recv()

        @pl.when(at < last)
        def _():
            copy.start()

    def gather_step(d, i):
        at = place[d]
        v = i - HOP_LAG * at

        @pl.when((v >= 0) & (v < 2 * early))
        def _():
            pass_on(early_copy(d, v), at)

        @pl.when((v >= 2 * early) & (v < gathers))
        def _():
            pass_on(late_copy(d, v), at)

    mine, other = rows(k * side_rows, side_rows), rows((1 - k) * side_rows, side_rows)
    cols_here, cols_there = rows(y * depth, depth), rows(yo * depth, depth)

    def k_copy(g):
        return remote(part.at[g, other, :], kgot.at[g], k_s.at[g], k_r.at[g], k_peer)

    def y_copy(g):
        return remote(ysend.at[g], ygot.at[g], y_s.at[g], y_r.at[g], y_peer)

    def x_copy(g):
        return remote(xsend.at[g], xgot.at[g], x_s.at[g], x_r.at[g], x_peer)

    def g_copy(g):
        ref = branch.at[g, mine, :]
        return remote(ref, ref, g_s.at[g], g_r.at[g], k_peer)

    def g_wait(g):
        ref = branch.at[g, other, :]
        remote(ref, ref, g_s.at[g], g_r.at[g], k_peer).wait_recv()

    def f_copy(b, step):
        peer = lax.rem(ra + step, n_ra)
        return remote(frow.at[b], fgot.at[b, ra], f_s.at[b, step], f_r.at[b, step], (peer, cb))

    def f_wait(b, step):
        src = lax.rem(ra + n_ra - step, n_ra)
        remote(frow.at[b], fgot.at[b, src], f_s.at[b, step], f_r.at[b, step], (src, cb)).wait_recv()

    def down_product(g):
        value = jnp.dot(hid[g], dwv[...], preferred_element_type=F32)
        part[g] = value.astype(BF16)
        keep[...] = value
        yown[g] = keep[mine, :]
        k_copy(g).start()

    def core_sum(g):
        k_copy(g).wait_recv()
        ysend[g] = (yown[g, :, cols_there] + kgot[g, :, cols_there].astype(F32)).astype(BF16)
        y_copy(g).start()

    def y_sum(g):
        y_copy(g).wait_recv()
        value = yown[g, :, cols_here] + kgot[g, :, cols_here].astype(F32) + ygot[g].astype(F32)
        xsend[g] = value.astype(BF16)
        x_copy(g).start()

    def x_sum(g):
        x_copy(g).wait_recv()
        branch[g, mine, :] = (xsend[g].astype(F32) + xgot[g].astype(F32)).astype(BF16)
        g_copy(g).start()

    def new_stream(g):
        g_wait(g)
        for side in range(2):
            r = slice(side * side_rows, (side + 1) * side_rows)
            old = tok[rows(side * half + g * side_rows, side_rows), :].astype(F32)
            stream[g, r, :] = 0.5 * old + branch[g, r, :].astype(F32)
        b, place_in = g // per_batch, lax.rem(g, per_batch)
        frow[b, pl.ds(place_in, 1), :] = row_sums(stream[g])

        @pl.when(place_in == per_batch - 1)
        def _():
            fgot[b, ra] = frow[b]
            for step in range(1, n_ra):
                f_copy(b, step).start()

    def finish(b):
        for step in range(1, n_ra):
            f_wait(b, step)
        total = fgot[b, 0]
        for r in range(1, n_ra):
            total = total + fgot[b, r]
        for e in range(per_batch):
            g = b * per_batch + e
            factor = spread(total[e : e + 1, :])
            for side in range(2):
                r = slice(side * side_rows, (side + 1) * side_rows)
                f = factor[r, :]
                to = rows(side * half + g * side_rows, side_rows)
                for c in range(depth // LANES):
                    cols = slice(c * LANES, (c + 1) * LANES)
                    out[to, cols] = (stream[g, r, cols] * f * out_gain[:, cols]).astype(BF16)

    def product(j):
        for e in range(2):
            w_keep(j, e).wait()
            w_wait(j, e)
        for b in range(nz):
            r = slice(b * block, (b + 1) * block)
            pbuf[lax.rem(j, 4), r, :] = jnp.dot(xf[r, :], wk[j], preferred_element_type=F32)

    reduce_end = messages + HOP_LAG * last
    gather_end = messages + gathers + HOP_LAG * last
    down_at = messages + 2 * early + HOP_LAG * last + DOWN_LAG
    stages = (down_product, core_sum, y_sum, x_sum, new_stream)
    names = ("down", "core_sum", "y_sum", "x_sum", "new_stream")
    turns = (0,) + STAGE_TURNS
    last_turn = groups + turns[-1]

    @pl.loop(0, down_at + 2 * last_turn)
    def _(i):
        @pl.when((lax.rem(i, STEPS) == 0) & (i < messages))
        def _():
            with jax.named_scope("product"):
                product(i // STEPS)

        @pl.when(i < reduce_end)
        def _():
            with jax.named_scope("reduce"):
                for d in range(2):
                    reduce_step(d, i)

        @pl.when((i >= messages) & (i < gather_end))
        def _():
            with jax.named_scope("gather"):
                for d in range(2):
                    gather_step(d, i - messages)

        behind = i - down_at
        t = behind // 2

        @pl.when((behind >= 0) & (lax.rem(behind, 2) == 0))
        def _():
            @pl.when(t == 0)
            def _():
                with jax.named_scope("down_wait"):
                    down_keep().wait()
                    down_wait()

            for turn, stage, name in reversed(list(zip(turns, stages, names))):
                @pl.when((t >= turn) & (t < groups + turn))
                def _():
                    with jax.named_scope(name):
                        stage(t - turn)

            for b in range(batches - 1):
                @pl.when(t == (b + 1) * per_batch + turns[-1] + 1)
                def _():
                    with jax.named_scope("finish"):
                        finish(b)

    with jax.named_scope("drain"):
        for kind in range(len(token_moves)):
            for p in range(PIECES):
                token_copy(kind, p).wait_send()
        down_send().wait_send()

        @pl.loop(0, chunks)
        def _(j):
            for i in range(2):
                w_send(j, i).wait_send()

        for d in range(2):
            @pl.when(place[d] < last)
            def _():
                c_copy(d).wait_send()

                @pl.loop(0, messages)
                def _(m):
                    r_copy(d, m).wait_send()

                @pl.loop(0, 2 * early)
                def _(v):
                    early_copy(d, v).wait_send()

                @pl.loop(2 * early, gathers)
                def _(v):
                    late_copy(d, v).wait_send()

        @pl.loop(0, groups)
        def _(g):
            for copy in (k_copy, y_copy, x_copy, g_copy):
                copy(g).wait_send()

    with jax.named_scope("finish"):
        finish(batches - 1)
    for b in range(batches):
        for step in range(1, n_ra):
            f_copy(b, step).wait_send()


def fused_body(nz, ny, n_cb, tokens, norm_gain, gate_weight, up_weight, down_weight, out_gain):
    n_tok, depth = tokens.shape
    n_ra = nz * ny
    units = gate_weight.shape[1] // ny
    chunks = units // LANES
    half = n_tok // 2
    messages = chunks * STEPS
    group = n_tok // GROUPS
    side = group // 2
    batches = 2
    gathers = 2 * (min(EARLY_CHUNKS, chunks - 1) + GROUPS)
    dma, vmem = pltpu.SemaphoreType.DMA, pltpu.VMEM
    scratch = [
        vmem((n_tok, ny * depth), BF16),
        vmem((chunks, ny * depth, LANES_PER_STEP), BF16),
        vmem((units, ny * depth), BF16),
        vmem((4, n_tok, LANES_PER_STEP), F32),
        vmem((2, messages, half // STEPS, LANES_PER_STEP), BF16),
        vmem((2, messages, half // STEPS, LANES_PER_STEP), BF16),
        vmem((half, LANES), F32),
        vmem((n_tok // LANES, LANES), F32),
        vmem((n_tok // LANES, LANES), F32),
        vmem((2, n_tok // LANES, LANES), F32),
        vmem((2, n_tok // LANES, LANES), F32),
        vmem((GROUPS, group, units), BF16),
        vmem((GROUPS, group, ny * depth), BF16),
        vmem((group, ny * depth), F32),
        vmem((GROUPS, side, ny * depth), BF16),
        vmem((GROUPS, side, ny * depth), F32),
        vmem((GROUPS, side, depth), BF16),
        vmem((GROUPS, side, depth), BF16),
        vmem((GROUPS, side, depth), BF16),
        vmem((GROUPS, side, depth), BF16),
        vmem((GROUPS, group, depth), BF16),
        vmem((GROUPS, group, depth), F32),
        vmem((batches, 8, LANES), F32),
        vmem((batches, n_ra, 8, LANES), F32),
        dma((4, PIECES)), dma((4, PIECES)), dma, dma, dma((2,)), dma((2,)),
        dma((chunks, 2)), dma((chunks, 2)), dma((chunks, 2)), dma, dma, dma,
        dma((2, messages)), dma((2, messages)), dma((2, gathers)), dma((2, gathers)),
        dma((GROUPS,)), dma((GROUPS,)), dma((GROUPS,)), dma((GROUPS,)),
        dma((GROUPS,)), dma((GROUPS,)), dma((GROUPS,)), dma((GROUPS,)),
        dma((batches, n_ra)), dma((batches, n_ra)),
    ]
    on_chip, anywhere = pl.BlockSpec(memory_space=vmem), pl.BlockSpec(memory_space=pl.ANY)
    return pl.pallas_call(
        functools.partial(fused_kernel, nz, ny, n_cb, depth * n_ra),
        out_shape=jax.ShapeDtypeStruct(tokens.shape, BF16),
        in_specs=[on_chip, on_chip, anywhere, anywhere, anywhere, on_chip],
        out_specs=on_chip,
        scratch_shapes=scratch,
        compiler_params=pltpu.CompilerParams(
            collective_id=0, has_side_effects=True, vmem_limit_bytes=64000 * 1024
        ),
    )(tokens, norm_gain[None, :], gate_weight, up_weight, down_weight, out_gain[None, :])


def solution(mesh):
    n_ra, n_cb = mesh.shape["ra"], mesh.shape["cb"]
    nz, ny = plane_sizes(mesh)
    plain = ring_body(mesh)

    def body(tokens, norm_gain, gate_weight, up_weight, down_weight, out_gain):
        args = (tokens, norm_gain, gate_weight, up_weight, down_weight, out_gain)
        whole = (
            nz == 4 and ny == 2 and n_cb == 4
            and gate_weight.shape[1] % (ny * LANES) == 0
            and tokens.shape[0] == GROUPS * LANES
            and tokens.shape[1] % LANES == 0
        )
        return fused_body(nz, ny, n_cb, *args) if whole else plain(*args)

    placed = (P(None, "ra"), P("ra"), P("ra", "cb"), P("ra", "cb"), P("cb", "ra"), P("ra"))
    return jax.shard_map(body, mesh=mesh, in_specs=placed, out_specs=P(None, "ra"), check_vma=False)
```

```python
import functools

import jax
import jax.numpy as jnp
from jax import lax
from jax.experimental import pallas as pl
from jax.experimental.pallas import tpu as pltpu
from jax.sharding import PartitionSpec as P

F32, BF16 = jnp.float32, jnp.bfloat16
MESH = pl.DeviceIdType.MESH
LANES = 128
LANES_PER_STEP = 2 * LANES
STEPS, GROUPS, PIECES = 4, 8, 2
EARLY_CHUNKS, HOP_LAG, DOWN_LAG = 3, 3, 4
RING, GATHER_RING, STAGE_RING = 16, 12, 8
FINISH_LAG = 3
STAGE_TURNS = (2, 5, 8, 10)
EPS = 1e-06


def plane_sizes(mesh):
    n = mesh.shape["ra"]
    column = mesh.devices[:, 0]
    coords = [getattr(d, "coords", None) for d in column]
    if all(c is not None for c in coords):
        ny = len({c[1] for c in coords})
    else:
        ny = 2 if n % 2 == 0 else 1
    return n // ny, ny


def ring_order(mesh):
    n = mesh.shape["ra"]
    column = mesh.devices[:, 0]
    coords = [getattr(d, "coords", None) for d in column]
    if all(c is not None for c in coords):
        ny = len({c[1] for c in coords})
    else:
        ny = 2 if n % 2 == 0 else 1
    nz = n // ny
    if ny == 1 or nz % 2 or nz * ny != n:
        return list(range(n))
    walk = []
    for z in range(nz):
        ys = range(1, ny) if z % 2 == 0 else range(ny - 1, 0, -1)
        walk += [z * ny + y for y in ys]
    return walk + [z * ny for z in reversed(range(nz))]


def butterfly(value, axis, n, narrow=None):
    if n & (n - 1):
        return lax.psum(value, axis)
    step = 1
    while step < n:
        sent = value if narrow is None else value.astype(narrow)
        got = lax.ppermute(sent, axis, [(i, i ^ step) for i in range(n)])
        value = sent.astype(F32) + got.astype(F32)
        step *= 2
    return value


def ring_body(mesh):
    n_ra, n_cb = mesh.shape["ra"], mesh.shape["cb"]
    order = ring_order(mesh)
    place = [order.index(i) for i in range(n_ra)]
    to_right = [(order[i], order[(i + 1) % n_ra]) for i in range(n_ra)]
    to_left = [(order[i], order[(i - 1) % n_ra]) for i in range(n_ra)]
    far = n_ra // 2

    def body(tokens, norm_gain, gate_weight, up_weight, down_weight, out_gain):
        rows = tokens.shape[0] // n_ra
        width = tokens.shape[1] * n_ra
        hidden_cols = gate_weight.shape[1]
        cut = -(-hidden_cols // 256) * 128
        cols = (slice(0, cut), slice(cut, hidden_cols))
        p = jnp.asarray(place, jnp.int32)[lax.axis_index("ra")]

        def block(array, b):
            start = lax.rem(p + b + n_ra, n_ra) * rows
            return lax.dynamic_slice_in_dim(array, start, rows, 0)

        stream_in = tokens.astype(F32)
        scaled = (stream_in * norm_gain[None, :]).astype(BF16)
        weights = {"g": gate_weight, "u": up_weight}

        def parts(source, offsets):
            x = jnp.concatenate([block(source, b) for b in offsets], axis=0)
            return {k: jnp.dot(x, w, preferred_element_type=F32) for k, w in weights.items()}

        right, left = {}, {}
        source = scaled
        for d in range(far, 0, -1):
            mine = parts(source, (d,) if d == far else (d, -d))
            if d < far:
                source, right["g"] = lax.optimization_barrier((source, right["g"]))
            for key in ("g", "u"):
                for flow, perm, skip, at in ((right, to_right, "u", 0), (left, to_left, "g", rows)):
                    if d == far and key == skip:
                        continue
                    value = mine[key] if d == far else mine[key][at : at + rows]
                    if key in flow:
                        value = value + flow[key].astype(F32)
                    flow[key] = lax.ppermute(value.astype(BF16), "ra", perm)
        mine = parts(source, (0,))

        squares = jnp.sum(stream_in * stream_in, axis=1)
        sq = block(squares, 0)
        for k in range(1, n_ra):
            perm = [(order[i], order[(i + k) % n_ra]) for i in range(n_ra)]
            sq = sq + lax.ppermute(block(squares, k), "ra", perm)
        inv_rms = lax.rsqrt(sq / width + 1e-06)[:, None]

        total = {}
        for key in ("g", "u"):
            value = mine[key]
            for flow in (right, left):
                if key in flow:
                    value = value + flow[key].astype(F32)
            total[key] = value * inv_rms
        own = (jax.nn.silu(total["g"]) * total["u"]).astype(BF16)

        stream = jnp.zeros(tokens.shape, F32)
        sums = jnp.zeros(tokens.shape[:1], F32)

        def finish(stream, sums, held):
            units = jnp.concatenate([h for _, h in held], axis=0)
            down = jnp.dot(units, down_weight, preferred_element_type=F32)
            branch = butterfly(down, "cb", n_cb, BF16)
            for i, (b, _) in enumerate(held):
                new = 0.5 * block(stream_in, b) + branch[i * rows : (i + 1) * rows]
                start = lax.rem(p + b + n_ra, n_ra) * rows
                stream = lax.dynamic_update_slice_in_dim(stream, new, start, 0)
                sums = lax.dynamic_update_slice_in_dim(sums, jnp.sum(new * new, axis=1), start, 0)
            return stream, sums

        from_left = from_right = own
        pending = [(0, own)]
        for s in range(1, far + 1):
            last = s == far
            if last:
                from_left, from_right = from_left[:, cols[0]], from_right[:, cols[1]]
            from_left = lax.ppermute(from_left, "ra", to_right)
            from_right = lax.ppermute(from_right, "ra", to_left)
            stream, sums = finish(stream, sums, pending)
            if last:
                pending = [(far, jnp.concatenate([from_left, from_right], axis=1))]
            else:
                pending = [(-s, from_left), (s, from_right)]
        stream, sums = finish(stream, sums, pending)

        total_sq = butterfly(sums, "ra", n_ra)
        factor = lax.rsqrt(total_sq / width + 1e-06)[:, None]
        return (stream * factor * out_gain[None, :]).astype(BF16)

    return body


def fused_kernel(
    nz, ny, n_cb, width,
    tok, gain, gate_w, up_w, down_w, out_gain, out,
    xf, wk, dwv, pbuf, rsend, rrecv, bown, bsend, bgot, inv, srow, speer, csend, crecv, hid,
    part, keep, kgot, yown, ysend, ygot, xsend, xgot, branch, stream, frow, fgot,
    tok_s, tok_r, sum_s, sum_r, c_s, c_r, wl, ws, wr, dl, ds, dr, b_s, b_r, r_s, r_r, h_s, h_r,
    k_s, k_r, y_s, y_r, x_s, x_r, g_s, g_r, f_s, f_r, obuf, o_s,
):
    n_ra = nz * ny
    tokens, depth = tok.shape
    chunks = wk.shape[0]
    half_cols = chunks * LANES
    half = tokens // 2
    step_rows = half // STEPS
    quarter = tokens // n_cb
    piece_rows = quarter // PIECES
    block = tokens // nz
    alone = chunks - 1
    messages = (chunks + 1) * STEPS
    groups, group, _ = hid.shape
    side_rows = group // 2
    batches = frow.shape[0]
    per_batch = groups // batches
    early = min(EARLY_CHUNKS, chunks - 1)
    gathers = 2 * (early + groups)

    ra, cb = lax.axis_index("ra"), lax.axis_index("cb")
    z, y = ra // ny, ra % ny
    yo = 1 - y
    x, k = cb // 2, cb % 2
    last = nz - 1
    y_peer = (z * ny + yo, cb)
    z_peer = (lax.rem(z + 1, nz) * ny + y, cb), (lax.rem(z + last, nz) * ny + y, cb)
    k_peer = (ra, x * 2 + 1 - k)
    x_peer = (ra, (1 - x) * 2 + k)
    place = (z, last - z)

    def remote(src, dst, send, recv, device):
        return pltpu.make_async_remote_copy(
            src_ref=src, dst_ref=dst, send_sem=send, recv_sem=recv, device_id=device, device_id_type=MESH
        )

    def rows(start, size):
        return pl.ds(pl.multiple_of(start, size), size)

    for side in range(2):
        for i, w in enumerate((gate_w, up_w)):
            cols = pl.ds(side * half_cols + alone * LANES, LANES)
            to = wk.at[alone, pl.ds(side * depth, depth), pl.ds(i * LANES, LANES)]
            pltpu.make_async_copy(w.at[:, cols], to, wl.at[0]).start()

    barrier = pltpu.get_barrier_semaphore()
    for peer in (y_peer, k_peer, x_peer):
        pl.semaphore_signal(barrier, inc=1, device_id=peer, device_id_type=MESH)
    for d in range(2):
        @pl.when(place[d] < last)
        def _():
            pl.semaphore_signal(barrier, inc=1, device_id=z_peer[d], device_id_type=MESH)

    def token_ref(q, p, side):
        return xf.at[rows(q * quarter + p * piece_rows, piece_rows), rows(side * depth, depth)]

    def scale(q, p):
        r = rows(q * quarter + p * piece_rows, piece_rows)
        xf[r, rows(y * depth, depth)] = (tok[r, :].astype(F32) * gain[...]).astype(BF16)

    xq = lax.rem(cb + 2, n_cb)
    kq = x * 2 + 1 - k
    kxq = (1 - x) * 2 + 1 - k
    token_moves = ((cb, y, y_peer), (cb, yo, x_peer), (cb, yo, k_peer), (xq, yo, k_peer))

    def token_copy(kind, p):
        q, side, device = token_moves[kind]
        recv = tok_r.at[2 * kind + p if kind < 2 else kind + 2]
        return remote(token_ref(q, p, side), token_ref(q, p, side), tok_s.at[kind], recv, device)

    def token_wait(kind, p):
        ref = token_ref((cb, xq)[kind], p, yo)
        remote(ref, ref, tok_s.at[kind], tok_r.at[2 * kind + p], y_peer).wait_recv()

    def token_quarter(kind, q, side):
        ref = xf.at[rows(q * quarter, quarter), rows(side * depth, depth)]
        return remote(ref, ref, tok_s.at[kind], tok_r.at[kind + 2], k_peer)

    def w_slot(j, i, side):
        return wk.at[j, rows(side * depth, depth), pl.ds(i * LANES, LANES)]

    def w_part(j, i, side):
        cols = pl.ds(pl.multiple_of(side * half_cols + j * LANES, LANES), LANES)
        return (gate_w, up_w)[i].at[:, cols]

    def w_send(j, i):
        return remote(w_part(j, i, yo), w_slot(j, i, y), ws, wr.at[j], y_peer)

    def w_sent():
        ref = wk.at[pl.ds(0, alone), rows(y * depth, depth), :]
        remote(ref, ref, ws, wr.at[0], y_peer).wait_send()

    def w_wait(j):
        ref = wk.at[j, rows(yo * depth, depth), :]
        remote(ref, ref, ws, wr.at[j], y_peer).wait_recv()

    def w_kept():
        ref = wk.at[pl.ds(0, alone), rows(y * depth, depth), :]
        pltpu.make_async_copy(ref, ref, wl.at[1]).wait()

    def alone_kept():
        ref = wk.at[alone]
        pltpu.make_async_copy(ref, ref, wl.at[0]).wait()

    def down_rows(side):
        return down_w.at[rows(side * half_cols, half_cols), :]

    down_here = dwv.at[:, rows(y * depth, depth)]
    down_there = dwv.at[:, rows(yo * depth, depth)]

    def down_send():
        return remote(down_rows(yo), down_here, ds, dr, y_peer)

    def down_wait():
        remote(down_there, down_there, ds, dr, y_peer).wait_recv()

    def down_keep():
        return pltpu.make_async_copy(down_rows(y), down_here, dl)

    def row_sums(value):
        square = value * value
        folded = square[:, :LANES]
        for c in range(1, depth // LANES):
            folded = folded + square[:, c * LANES : (c + 1) * LANES]
        return jnp.sum(jnp.transpose(folded), axis=0, keepdims=True)

    def spread(row):
        return jnp.transpose(jnp.broadcast_to(lax.rsqrt(row / width + EPS), (LANES, LANES)))

    def sum_copy():
        return remote(srow, speer, sum_s, sum_r, y_peer)

    for p in range(PIECES):
        scale(cb, p)
    pl.semaphore_wait(barrier, 3 + jnp.minimum(z, 1) + jnp.minimum(last - z, 1))
    with jax.named_scope("scale"):
        for p in range(PIECES):
            token_copy(0, p).start()
        for step in range(1, n_cb):
            for p in range(PIECES):
                scale(lax.rem(cb + step, n_cb), p)
    with jax.named_scope("sums"):
        for b in range(tokens // LANES):
            srow[b : b + 1, :] = row_sums(tok[b * LANES : (b + 1) * LANES, :].astype(F32))
        sum_copy().start()
    frow[...] = jnp.zeros_like(frow)

    with jax.named_scope("issue"):
        @pl.loop(0, alone)
        def _(j):
            for i in range(2):
                w_send(j, i).start()

        @pl.loop(0, alone)
        def _(j):
            for i in range(2):
                pltpu.make_async_copy(w_part(j, i, y), w_slot(j, i, y), wl.at[1]).start()

        down_keep().start()

    def r_copy(d, m):
        return remote(rsend.at[d, m], rrecv.at[d, m], r_s.at[d], r_r.at[d, lax.rem(m, RING)], z_peer[d])

    def c_copy(d):
        return remote(csend.at[d], crecv.at[d], c_s.at[d], c_r.at[d], z_peer[d])

    def hidden_block(d, j, q, value):
        factor = inv[rows(q * step_rows, step_rows), :]
        gate = value[:, :LANES] * factor
        up = value[:, LANES:] * factor
        hidden = (gate / (1.0 + jnp.exp(-gate)) * up).astype(BF16)
        per = step_rows // side_rows
        for s in range(per):
            cols = rows(j * LANES, LANES)
            hid[q * per + s, pl.ds((1 - d) * side_rows, side_rows), cols] = hidden[s * side_rows : (s + 1) * side_rows]

    def reduce_step(d, i):
        at = place[d]
        m = i - HOP_LAG * at
        start = (1 - d) * half

        @pl.when((m >= 0) & (m < messages))
        def _():
            j, q = m // STEPS, lax.rem(m, STEPS)
            slot = lax.rem(j, 4)
            r = rows(start + q * step_rows, step_rows)

            @pl.when(at == 0)
            def _():
                @pl.when(m == 2 * STEPS)
                def _():
                    csend[d] = srow[...]
                    c_copy(d).start()

                rsend[d, m] = pbuf[slot, r, :].astype(BF16)
                r_copy(d, m).start()

            @pl.when((at > 0) & (at < last))
            def _():
                @pl.when(m == 2 * STEPS)
                def _():
                    c_copy(d).wait_recv()
                    csend[d] = srow[...] + crecv[d]
                    c_copy(d).start()

                r_copy(d, m).wait_recv()
                rsend[d, m] = (pbuf[slot, r, :] + rrecv[d, m].astype(F32)).astype(BF16)
                r_copy(d, m).start()

            @pl.when(at == last)
            def _():
                @pl.when(m == 2 * STEPS)
                def _():
                    c_copy(d).wait_recv()
                    total = srow[...] + crecv[d]
                    for b in range(half // LANES):
                        row = start // LANES + b
                        inv[b * LANES : (b + 1) * LANES, :] = spread(total[row : row + 1, :])

                r_copy(d, m).wait_recv()
                value = pbuf[slot, r, :] + rrecv[d, m].astype(F32)

                @pl.when(j >= 2)
                def _():
                    hidden_block(d, j - 2, q, value)

                @pl.when(j == y)
                def _():
                    bown[q] = value

                @pl.when(j == yo)
                def _():
                    bsend[q] = value.astype(BF16)
                    remote(bsend.at[q], bgot.at[q], b_s, b_r, y_peer).start()

    def alone_copy():
        return remote(bsend, bgot, b_s, b_r, y_peer)

    def alone_hidden(q):
        @pl.when(q == 0)
        def _():
            alone_copy().wait_recv()

        for d in range(2):
            @pl.when(place[d] == last)
            def _():
                hidden_block(d, alone, q, bown[q] + bgot[q].astype(F32))

    def early_copy(d, v):
        lower = groups // 2
        ref = hid.at[rows(lax.rem(v, 2) * lower, lower), pl.ds(d * side_rows, side_rows), rows(v // 2 * LANES, LANES)]
        return remote(ref, ref, h_s.at[d], h_r.at[d, lax.rem(v, GATHER_RING)], z_peer[d])

    def late_copy(d, v):
        u = v - 2 * early
        lower = side_rows // 2
        r = rows(d * side_rows + lax.rem(u, 2) * lower, lower)
        ref = hid.at[u // 2, r, pl.ds(early * LANES, (chunks - early) * LANES)]
        return remote(ref, ref, h_s.at[d], h_r.at[d, lax.rem(v, GATHER_RING)], z_peer[d])

    def pass_on(copy, at):
        @pl.when(at > 0)
        def _():
            copy.wait_recv()

        @pl.when(at < last)
        def _():
            copy.start()

    def gather_step(d, i):
        at = place[d]
        v = i - HOP_LAG * at

        @pl.when((v >= 0) & (v < 2 * early))
        def _():
            pass_on(early_copy(d, v), at)

        @pl.when((v >= 2 * early) & (v < gathers))
        def _():
            pass_on(late_copy(d, v), at)

    mine, other = rows(k * side_rows, side_rows), rows((1 - k) * side_rows, side_rows)
    cols_here, cols_there = rows(y * depth, depth), rows(yo * depth, depth)

    def k_copy(g):
        return remote(part.at[g, other, :], kgot.at[g], k_s, k_r.at[lax.rem(g, STAGE_RING)], k_peer)

    def y_copy(g):
        return remote(ysend.at[g], ygot.at[g], y_s, y_r.at[lax.rem(g, STAGE_RING)], y_peer)

    def x_copy(g):
        return remote(xsend.at[g], xgot.at[g], x_s, x_r.at[lax.rem(g, STAGE_RING)], x_peer)

    def g_copy(g):
        ref = branch.at[g, mine, :]
        return remote(ref, ref, g_s, g_r.at[lax.rem(g, STAGE_RING)], k_peer)

    def g_wait(g):
        ref = branch.at[g, other, :]
        remote(ref, ref, g_s, g_r.at[lax.rem(g, STAGE_RING)], k_peer).wait_recv()

    def f_copy(b, step):
        peer = lax.rem(ra + step, n_ra)
        return remote(frow.at[b], fgot.at[b, step - 1], f_s.at[b], f_r.at[b], (peer, cb))

    def f_all(b):
        return remote(fgot.at[b], fgot.at[b], f_s.at[b], f_r.at[b], y_peer)

    def down_product(g):
        value = jnp.dot(hid[g], dwv[...], preferred_element_type=F32)
        part[g] = value.astype(BF16)
        keep[...] = value
        yown[g] = keep[mine, :]
        k_copy(g).start()

    def core_sum(g):
        k_copy(g).wait_recv()
        ysend[g] = (yown[g, :, cols_there] + kgot[g, :, cols_there].astype(F32)).astype(BF16)
        y_copy(g).start()

    def y_sum(g):
        y_copy(g).wait_recv()
        value = yown[g, :, cols_here] + kgot[g, :, cols_here].astype(F32) + ygot[g].astype(F32)
        xsend[g] = value.astype(BF16)
        x_copy(g).start()

    def x_sum(g):
        x_copy(g).wait_recv()
        branch[g, mine, :] = (xsend[g].astype(F32) + xgot[g].astype(F32)).astype(BF16)
        g_copy(g).start()

    def new_stream(g):
        g_wait(g)
        for side in range(2):
            r = slice(side * side_rows, (side + 1) * side_rows)
            old = tok[rows(side * half + g * side_rows, side_rows), :].astype(F32)
            stream[g, r, :] = 0.5 * old + branch[g, r, :].astype(F32)
        b, place_in = g // per_batch, lax.rem(g, per_batch)
        frow[b, pl.ds(place_in, 1), :] = row_sums(stream[g])

        @pl.when(place_in == per_batch - 1)
        def _():
            for step in range(1, n_ra):
                f_copy(b, step).start()

    def out_copy(g, side):
        r = rows(side * half + g * side_rows, side_rows)
        return pltpu.make_async_copy(obuf.at[r, :], out.at[r, :], o_s)

    def finish(b):
        f_all(b).wait_recv()
        total = frow[b]
        for r in range(n_ra - 1):
            total = total + fgot[b, r]
        for e in range(per_batch):
            g = b * per_batch + e
            factor = spread(total[e : e + 1, :])
            for side in range(2):
                r = slice(side * side_rows, (side + 1) * side_rows)
                f = factor[r, :]
                to = rows(side * half + g * side_rows, side_rows)
                for c in range(depth // LANES):
                    cols = slice(c * LANES, (c + 1) * LANES)
                    obuf[to, cols] = (stream[g, r, cols] * f * out_gain[:, cols]).astype(BF16)
                out_copy(g, side).start()

    def product(j):
        @pl.when(j == 0)
        def _():
            alone_kept()

        @pl.when(j < 2)
        def _():
            for b in range(nz):
                r = slice(b * block, (b + 1) * block)
                pbuf[j, r, :] = jnp.dot(
                    xf[r, cols_here], wk[alone, rows(j * depth, depth), :], preferred_element_type=F32
                )

        @pl.when(j == 2)
        def _():
            for p in range(PIECES):
                token_wait(1, p)
                token_copy(3, p).start()
            token_quarter(2, kq, yo).wait_recv()
            token_quarter(3, kxq, yo).wait_recv()
            sum_copy().wait()
            srow[...] = srow[...] + speer[...]
            w_kept()

        @pl.when(j >= 2)
        def _():
            w_wait(j - 2)
            for b in range(nz):
                r = slice(b * block, (b + 1) * block)
                pbuf[lax.rem(j, 4), r, :] = jnp.dot(xf[r, :], wk[j - 2], preferred_element_type=F32)

    def tokens_on(p):
        token_wait(0, p)
        token_copy(1, p).start()
        token_copy(2, p).start()

    reduce_end = messages + HOP_LAG * last
    gather_end = messages + gathers + HOP_LAG * last
    ready = messages + 2 * early + HOP_LAG * last + 1
    stages = (down_product, core_sum, y_sum, x_sum, new_stream)
    names = ("down", "core_sum", "y_sum", "x_sum", "new_stream")
    turns = (0,) + STAGE_TURNS
    loop_end = ready + 2 * groups - 1 + turns[-1]

    @pl.loop(0, loop_end)
    def _(i):
        @pl.when((lax.rem(i, STEPS) == 0) & (i < messages))
        def _():
            with jax.named_scope("product"):
                product(i // STEPS)

        for p in range(PIECES):
            @pl.when(i == 2 * p + 3)
            def _():
                with jax.named_scope("tokens"):
                    tokens_on(p)

        @pl.when(i == 2 * STEPS + HOP_LAG * last + 1)
        def _():
            down_send().start()

        @pl.when((i >= messages) & (i < messages + STEPS) & ((z == 0) | (z == last)))
        def _():
            with jax.named_scope("alone"):
                alone_hidden(i - messages)

        @pl.when(i < reduce_end)
        def _():
            with jax.named_scope("reduce"):
                for d in range(2):
                    reduce_step(d, i)

        @pl.when((i >= messages) & (i < gather_end))
        def _():
            with jax.named_scope("gather"):
                for d in range(2):
                    gather_step(d, i - messages)

        def on_turn(offset):
            s = i - ready - offset
            soon = s < 2 * DOWN_LAG
            g = jnp.where(soon, s - DOWN_LAG, s // 2)
            return g, (g >= 0) & (g < groups) & (soon | (lax.rem(s, 2) == 0))

        @pl.when(i >= ready)
        def _():
            @pl.when(i == ready + DOWN_LAG)
            def _():
                with jax.named_scope("down_wait"):
                    down_keep().wait()
                    down_wait()

            for turn, stage, name in reversed(list(zip(turns, stages, names))):
                g, due = on_turn(turn)

                @pl.when(due)
                def _():
                    with jax.named_scope(name):
                        stage(g)

            for b in range(batches - 1):
                g, due = on_turn(turns[-1] + FINISH_LAG)

                @pl.when(due & (g == (b + 1) * per_batch - 1))
                def _():
                    with jax.named_scope("finish"):
                        finish(b)

    with jax.named_scope("drain"):
        for kind, (q, side) in enumerate(((cb, y), (cb, yo), (cb, yo), (xq, yo))):
            token_quarter(kind, q, side).wait_send()
        down_send().wait_send()
        w_sent()

        @pl.when((z == 0) | (z == last))
        def _():
            alone_copy().wait_send()

        for d in range(2):
            @pl.when(place[d] < last)
            def _():
                c_copy(d).wait_send()
                remote(rsend.at[d], rrecv.at[d], r_s.at[d], r_r.at[d, 0], z_peer[d]).wait_send()
                ref = hid.at[:, pl.ds(d * side_rows, side_rows), :]
                remote(ref, ref, h_s.at[d], h_r.at[d, 0], z_peer[d]).wait_send()

        remote(kgot, kgot, k_s, k_r.at[0], k_peer).wait_send()
        remote(ygot, ygot, y_s, y_r.at[0], y_peer).wait_send()
        remote(xgot, xgot, x_s, x_r.at[0], x_peer).wait_send()
        ref = branch.at[:, mine, :]
        remote(ref, ref, g_s, g_r.at[0], k_peer).wait_send()

    with jax.named_scope("finish"):
        finish(batches - 1)
    with jax.named_scope("sent"):
        for b in range(batches):
            f_all(b).wait_send()
        pltpu.make_async_copy(obuf, out, o_s).wait()


def fused_body(nz, ny, n_cb, tokens, norm_gain, gate_weight, up_weight, down_weight, out_gain):
    n_tok, depth = tokens.shape
    n_ra = nz * ny
    units = gate_weight.shape[1] // ny
    chunks = units // LANES
    half = n_tok // 2
    messages = (chunks + 1) * STEPS
    group = n_tok // GROUPS
    side = group // 2
    batches = 2
    dma, vmem = pltpu.SemaphoreType.DMA, pltpu.VMEM
    scratch = [
        vmem((n_tok, ny * depth), BF16),
        vmem((chunks, ny * depth, LANES_PER_STEP), BF16),
        vmem((units, ny * depth), BF16),
        vmem((4, n_tok, LANES_PER_STEP), F32),
        vmem((2, messages, half // STEPS, LANES_PER_STEP), BF16),
        vmem((2, messages, half // STEPS, LANES_PER_STEP), BF16),
        vmem((STEPS, half // STEPS, LANES_PER_STEP), F32),
        vmem((STEPS, half // STEPS, LANES_PER_STEP), BF16),
        vmem((STEPS, half // STEPS, LANES_PER_STEP), BF16),
        vmem((half, LANES), F32),
        vmem((n_tok // LANES, LANES), F32),
        vmem((n_tok // LANES, LANES), F32),
        vmem((2, n_tok // LANES, LANES), F32),
        vmem((2, n_tok // LANES, LANES), F32),
        vmem((GROUPS, group, units), BF16),
        vmem((GROUPS, group, ny * depth), BF16),
        vmem((group, ny * depth), F32),
        vmem((GROUPS, side, ny * depth), BF16),
        vmem((GROUPS, side, ny * depth), F32),
        vmem((GROUPS, side, depth), BF16),
        vmem((GROUPS, side, depth), BF16),
        vmem((GROUPS, side, depth), BF16),
        vmem((GROUPS, side, depth), BF16),
        vmem((GROUPS, group, depth), BF16),
        vmem((GROUPS, group, depth), F32),
        vmem((batches, 8, LANES), F32),
        vmem((batches, n_ra - 1, 8, LANES), F32),
        dma((4,)), dma((6,)), dma, dma, dma((2,)), dma((2,)),
        dma((2,)), dma, dma((chunks - 1,)), dma, dma, dma, dma, dma,
        dma((2,)), dma((2, RING)), dma((2,)), dma((2, GATHER_RING)),
        dma, dma((STAGE_RING,)), dma, dma((STAGE_RING,)), dma, dma((STAGE_RING,)), dma, dma((STAGE_RING,)),
        dma((batches,)), dma((batches,)), vmem(tokens.shape, BF16), dma,
    ]
    on_chip, anywhere = pl.BlockSpec(memory_space=vmem), pl.BlockSpec(memory_space=pl.ANY)
    return pl.pallas_call(
        functools.partial(fused_kernel, nz, ny, n_cb, depth * n_ra),
        out_shape=jax.ShapeDtypeStruct(tokens.shape, BF16),
        in_specs=[on_chip, on_chip, anywhere, anywhere, anywhere, on_chip],
        out_specs=anywhere,
        scratch_shapes=scratch,
        compiler_params=pltpu.CompilerParams(
            collective_id=0, has_side_effects=True, vmem_limit_bytes=64000 * 1024
        ),
    )(tokens, norm_gain[None, :], gate_weight, up_weight, down_weight, out_gain[None, :])


def solution(mesh):
    n_ra, n_cb = mesh.shape["ra"], mesh.shape["cb"]
    nz, ny = plane_sizes(mesh)
    plain = ring_body(mesh)

    def body(tokens, norm_gain, gate_weight, up_weight, down_weight, out_gain):
        args = (tokens, norm_gain, gate_weight, up_weight, down_weight, out_gain)
        whole = (
            nz == 4 and ny == 2 and n_cb == 4
            and gate_weight.shape[1] % (ny * LANES) == 0
            and tokens.shape[0] == GROUPS * LANES
            and tokens.shape[1] % LANES == 0
        )
        return fused_body(nz, ny, n_cb, *args) if whole else plain(*args)

    placed = (P(None, "ra"), P("ra"), P("ra", "cb"), P("ra", "cb"), P("cb", "ra"), P("ra"))
    return jax.shard_map(body, mesh=mesh, in_specs=placed, out_specs=P(None, "ra"), check_vma=False)
```

```python
import functools

import jax
import jax.numpy as jnp
from jax import lax
from jax.experimental import pallas as pl
from jax.experimental.pallas import tpu as pltpu
from jax.sharding import PartitionSpec as P

F32, BF16 = jnp.float32, jnp.bfloat16
MESH = pl.DeviceIdType.MESH
LANES = 128
LANES_PER_STEP = 2 * LANES
STEPS, GROUPS, PIECES = 4, 8, 2
EARLY_CHUNKS, HOP_LAG, DOWN_LAG = 3, 3, 4
RING, GATHER_RING, STAGE_RING = 16, 12, 8
FINISH_LAG = 3
STAGE_TURNS = (2, 5, 9, 11)
EPS = 1e-06


def plane_sizes(mesh):
    n = mesh.shape["ra"]
    column = mesh.devices[:, 0]
    coords = [getattr(d, "coords", None) for d in column]
    if all(c is not None for c in coords):
        ny = len({c[1] for c in coords})
    else:
        ny = 2 if n % 2 == 0 else 1
    return n // ny, ny


def ring_order(mesh):
    n = mesh.shape["ra"]
    column = mesh.devices[:, 0]
    coords = [getattr(d, "coords", None) for d in column]
    if all(c is not None for c in coords):
        ny = len({c[1] for c in coords})
    else:
        ny = 2 if n % 2 == 0 else 1
    nz = n // ny
    if ny == 1 or nz % 2 or nz * ny != n:
        return list(range(n))
    walk = []
    for z in range(nz):
        ys = range(1, ny) if z % 2 == 0 else range(ny - 1, 0, -1)
        walk += [z * ny + y for y in ys]
    return walk + [z * ny for z in reversed(range(nz))]


def butterfly(value, axis, n, narrow=None):
    if n & (n - 1):
        return lax.psum(value, axis)
    step = 1
    while step < n:
        sent = value if narrow is None else value.astype(narrow)
        got = lax.ppermute(sent, axis, [(i, i ^ step) for i in range(n)])
        value = sent.astype(F32) + got.astype(F32)
        step *= 2
    return value


def ring_body(mesh):
    n_ra, n_cb = mesh.shape["ra"], mesh.shape["cb"]
    order = ring_order(mesh)
    place = [order.index(i) for i in range(n_ra)]
    to_right = [(order[i], order[(i + 1) % n_ra]) for i in range(n_ra)]
    to_left = [(order[i], order[(i - 1) % n_ra]) for i in range(n_ra)]
    far = n_ra // 2

    def body(tokens, norm_gain, gate_weight, up_weight, down_weight, out_gain):
        rows = tokens.shape[0] // n_ra
        width = tokens.shape[1] * n_ra
        hidden_cols = gate_weight.shape[1]
        cut = -(-hidden_cols // 256) * 128
        cols = (slice(0, cut), slice(cut, hidden_cols))
        p = jnp.asarray(place, jnp.int32)[lax.axis_index("ra")]

        def block(array, b):
            start = lax.rem(p + b + n_ra, n_ra) * rows
            return lax.dynamic_slice_in_dim(array, start, rows, 0)

        stream_in = tokens.astype(F32)
        scaled = (stream_in * norm_gain[None, :]).astype(BF16)
        weights = {"g": gate_weight, "u": up_weight}

        def parts(source, offsets):
            x = jnp.concatenate([block(source, b) for b in offsets], axis=0)
            return {k: jnp.dot(x, w, preferred_element_type=F32) for k, w in weights.items()}

        right, left = {}, {}
        source = scaled
        for d in range(far, 0, -1):
            mine = parts(source, (d,) if d == far else (d, -d))
            if d < far:
                source, right["g"] = lax.optimization_barrier((source, right["g"]))
            for key in ("g", "u"):
                for flow, perm, skip, at in ((right, to_right, "u", 0), (left, to_left, "g", rows)):
                    if d == far and key == skip:
                        continue
                    value = mine[key] if d == far else mine[key][at : at + rows]
                    if key in flow:
                        value = value + flow[key].astype(F32)
                    flow[key] = lax.ppermute(value.astype(BF16), "ra", perm)
        mine = parts(source, (0,))

        squares = jnp.sum(stream_in * stream_in, axis=1)
        sq = block(squares, 0)
        for k in range(1, n_ra):
            perm = [(order[i], order[(i + k) % n_ra]) for i in range(n_ra)]
            sq = sq + lax.ppermute(block(squares, k), "ra", perm)
        inv_rms = lax.rsqrt(sq / width + 1e-06)[:, None]

        total = {}
        for key in ("g", "u"):
            value = mine[key]
            for flow in (right, left):
                if key in flow:
                    value = value + flow[key].astype(F32)
            total[key] = value * inv_rms
        own = (jax.nn.silu(total["g"]) * total["u"]).astype(BF16)

        stream = jnp.zeros(tokens.shape, F32)
        sums = jnp.zeros(tokens.shape[:1], F32)

        def finish(stream, sums, held):
            units = jnp.concatenate([h for _, h in held], axis=0)
            down = jnp.dot(units, down_weight, preferred_element_type=F32)
            branch = butterfly(down, "cb", n_cb, BF16)
            for i, (b, _) in enumerate(held):
                new = 0.5 * block(stream_in, b) + branch[i * rows : (i + 1) * rows]
                start = lax.rem(p + b + n_ra, n_ra) * rows
                stream = lax.dynamic_update_slice_in_dim(stream, new, start, 0)
                sums = lax.dynamic_update_slice_in_dim(sums, jnp.sum(new * new, axis=1), start, 0)
            return stream, sums

        from_left = from_right = own
        pending = [(0, own)]
        for s in range(1, far + 1):
            last = s == far
            if last:
                from_left, from_right = from_left[:, cols[0]], from_right[:, cols[1]]
            from_left = lax.ppermute(from_left, "ra", to_right)
            from_right = lax.ppermute(from_right, "ra", to_left)
            stream, sums = finish(stream, sums, pending)
            if last:
                pending = [(far, jnp.concatenate([from_left, from_right], axis=1))]
            else:
                pending = [(-s, from_left), (s, from_right)]
        stream, sums = finish(stream, sums, pending)

        total_sq = butterfly(sums, "ra", n_ra)
        factor = lax.rsqrt(total_sq / width + 1e-06)[:, None]
        return (stream * factor * out_gain[None, :]).astype(BF16)

    return body


def fused_kernel(
    nz, ny, n_cb, width,
    tok_in, gain_in, gate_w, up_w, down_w, out_gain_in, out,
    xf, wk, dwv, pbuf, rsend, rrecv, bown, bsend, bgot, inv, srow, speer, csend, crecv, hid,
    part, keep, kgot, yown, ysend, ygot, xsend, xgot, branch, stream, frow, fgot,
    tok_s, tok_r, sum_s, sum_r, c_s, c_r, wl, ws, wr, dl, ds, dr, b_s, b_r, r_s, r_r, h_s, h_r,
    k_s, k_r, y_s, y_r, x_s, x_r, g_s, g_r, f_s, f_r, obuf, o_s, folds, tok, gain, out_gain, i_s,
):
    arrivals = [
        pltpu.make_async_copy(src, dst, i_s.at[n])
        for n, (src, dst) in enumerate(((tok_in, tok), (gain_in, gain), (out_gain_in, out_gain)))
    ]
    for copy in arrivals:
        copy.start()
    n_ra = nz * ny
    tokens, depth = tok.shape
    chunks = wk.shape[0]
    half_cols = chunks * LANES
    half = tokens // 2
    step_rows = half // STEPS
    quarter = tokens // n_cb
    piece_rows = quarter // PIECES
    block = tokens // nz
    alone = chunks - 1
    messages = (chunks + 1) * STEPS
    groups, group, _ = hid.shape
    side_rows = group // 2
    batches = frow.shape[0]
    per_batch = groups // batches
    early = min(EARLY_CHUNKS, chunks - 1)
    gathers = 2 * (early + groups)

    ra, cb = lax.axis_index("ra"), lax.axis_index("cb")
    z, y = ra // ny, ra % ny
    yo = 1 - y
    x, k = cb // 2, cb % 2
    last = nz - 1
    y_peer = (z * ny + yo, cb)
    z_peer = (lax.rem(z + 1, nz) * ny + y, cb), (lax.rem(z + last, nz) * ny + y, cb)
    k_peer = (ra, x * 2 + 1 - k)
    x_peer = (ra, (1 - x) * 2 + k)
    place = (z, last - z)

    def remote(src, dst, send, recv, device):
        return pltpu.make_async_remote_copy(
            src_ref=src, dst_ref=dst, send_sem=send, recv_sem=recv, device_id=device, device_id_type=MESH
        )

    def rows(start, size):
        return pl.ds(pl.multiple_of(start, size), size)

    for side in range(2):
        for i, w in enumerate((gate_w, up_w)):
            cols = pl.ds(side * half_cols + alone * LANES, LANES)
            to = wk.at[alone, pl.ds(side * depth, depth), pl.ds(i * LANES, LANES)]
            pltpu.make_async_copy(w.at[:, cols], to, wl.at[0]).start()

    barrier = pltpu.get_barrier_semaphore()
    for peer in (y_peer, k_peer, x_peer):
        pl.semaphore_signal(barrier, inc=1, device_id=peer, device_id_type=MESH)
    for d in range(2):
        @pl.when(place[d] < last)
        def _():
            pl.semaphore_signal(barrier, inc=1, device_id=z_peer[d], device_id_type=MESH)

    def token_ref(q, p, side):
        return xf.at[rows(q * quarter + p * piece_rows, piece_rows), rows(side * depth, depth)]

    def scale(q, p):
        r = rows(q * quarter + p * piece_rows, piece_rows)
        xf[r, rows(y * depth, depth)] = (tok[r, :].astype(F32) * gain[...]).astype(BF16)

    xq = lax.rem(cb + 2, n_cb)
    kq = x * 2 + 1 - k
    kxq = (1 - x) * 2 + 1 - k
    token_moves = ((cb, y, y_peer), (cb, yo, x_peer), (cb, yo, k_peer), (xq, yo, k_peer))

    def token_copy(kind, p):
        q, side, device = token_moves[kind]
        recv = tok_r.at[2 * kind + p if kind < 2 else kind + 2]
        return remote(token_ref(q, p, side), token_ref(q, p, side), tok_s.at[kind], recv, device)

    def token_wait(kind, p):
        ref = token_ref((cb, xq)[kind], p, yo)
        remote(ref, ref, tok_s.at[kind], tok_r.at[2 * kind + p], y_peer).wait_recv()

    def token_quarter(kind, q, side):
        ref = xf.at[rows(q * quarter, quarter), rows(side * depth, depth)]
        return remote(ref, ref, tok_s.at[kind], tok_r.at[kind + 2], k_peer)

    def w_slot(j, i, side):
        return wk.at[j, rows(side * depth, depth), pl.ds(i * LANES, LANES)]

    def w_part(j, i, side):
        cols = pl.ds(pl.multiple_of(side * half_cols + j * LANES, LANES), LANES)
        return (gate_w, up_w)[i].at[:, cols]

    def w_send(j, i):
        return remote(w_part(j, i, yo), w_slot(j, i, y), ws, wr.at[j], y_peer)

    def w_sent():
        ref = wk.at[pl.ds(0, alone), rows(y * depth, depth), :]
        remote(ref, ref, ws, wr.at[0], y_peer).wait_send()

    def w_wait(j):
        ref = wk.at[j, rows(yo * depth, depth), :]
        remote(ref, ref, ws, wr.at[j], y_peer).wait_recv()

    def w_kept():
        ref = wk.at[pl.ds(0, alone), rows(y * depth, depth), :]
        pltpu.make_async_copy(ref, ref, wl.at[1]).wait()

    def alone_kept():
        ref = wk.at[alone]
        pltpu.make_async_copy(ref, ref, wl.at[0]).wait()

    def down_rows(side):
        return down_w.at[rows(side * half_cols, half_cols), :]

    down_here = dwv.at[:, rows(y * depth, depth)]
    down_there = dwv.at[:, rows(yo * depth, depth)]

    def down_send():
        return remote(down_rows(yo), down_here, ds, dr, y_peer)

    def down_wait():
        remote(down_there, down_there, ds, dr, y_peer).wait_recv()

    def down_keep():
        return pltpu.make_async_copy(down_rows(y), down_here, dl)

    def fold(value):
        square = value * value
        folded = square[:, :LANES]
        for c in range(1, depth // LANES):
            folded = folded + square[:, c * LANES : (c + 1) * LANES]
        return folded

    def row_sums(value):
        return jnp.sum(jnp.transpose(fold(value)), axis=0, keepdims=True)

    def spread(row):
        return jnp.transpose(jnp.broadcast_to(lax.rsqrt(row / width + EPS), (LANES, LANES)))

    def sum_copy():
        return remote(srow, speer, sum_s, sum_r, y_peer)

    for copy in arrivals:
        copy.wait()
    for p in range(PIECES):
        scale(cb, p)
    pl.semaphore_wait(barrier, 3 + jnp.minimum(z, 1) + jnp.minimum(last - z, 1))
    with jax.named_scope("scale"):
        for p in range(PIECES):
            token_copy(0, p).start()
        for step in range(1, n_cb):
            for p in range(PIECES):
                scale(lax.rem(cb + step, n_cb), p)
    with jax.named_scope("sums"):
        for b in range(tokens // LANES):
            srow[b : b + 1, :] = row_sums(tok[b * LANES : (b + 1) * LANES, :].astype(F32))
        sum_copy().start()
    frow[...] = jnp.zeros_like(frow)

    with jax.named_scope("issue"):
        @pl.loop(0, alone)
        def _(j):
            for i in range(2):
                w_send(j, i).start()

        @pl.loop(0, alone)
        def _(j):
            for i in range(2):
                pltpu.make_async_copy(w_part(j, i, y), w_slot(j, i, y), wl.at[1]).start()

        down_keep().start()

    def r_copy(d, m):
        return remote(rsend.at[d, m], rrecv.at[d, m], r_s.at[d], r_r.at[d, lax.rem(m, RING)], z_peer[d])

    def c_copy(d):
        return remote(csend.at[d], crecv.at[d], c_s.at[d], c_r.at[d], z_peer[d])

    def hidden_block(d, j, q, value):
        factor = inv[rows(q * step_rows, step_rows), :]
        gate = value[:, :LANES] * factor
        up = value[:, LANES:] * factor
        hidden = (gate / (1.0 + jnp.exp(-gate)) * up).astype(BF16)
        per = step_rows // side_rows
        for s in range(per):
            cols = rows(j * LANES, LANES)
            hid[q * per + s, pl.ds((1 - d) * side_rows, side_rows), cols] = hidden[s * side_rows : (s + 1) * side_rows]

    def reduce_step(d, i):
        at = place[d]
        m = i - HOP_LAG * at
        start = (1 - d) * half

        @pl.when((m >= 0) & (m < messages))
        def _():
            j, q = m // STEPS, lax.rem(m, STEPS)
            slot = lax.rem(j, 4)
            r = rows(start + q * step_rows, step_rows)

            @pl.when(at == 0)
            def _():
                @pl.when(m == 2 * STEPS)
                def _():
                    csend[d] = srow[...]
                    c_copy(d).start()

                rsend[d, m] = pbuf[slot, r, :].astype(BF16)
                r_copy(d, m).start()

            @pl.when((at > 0) & (at < last))
            def _():
                @pl.when(m == 2 * STEPS)
                def _():
                    c_copy(d).wait_recv()
                    csend[d] = srow[...] + crecv[d]
                    c_copy(d).start()

                r_copy(d, m).wait_recv()
                rsend[d, m] = (pbuf[slot, r, :] + rrecv[d, m].astype(F32)).astype(BF16)
                r_copy(d, m).start()

            @pl.when(at == last)
            def _():
                @pl.when(m == 2 * STEPS)
                def _():
                    c_copy(d).wait_recv()
                    total = srow[...] + crecv[d]
                    for b in range(half // LANES):
                        row = start // LANES + b
                        inv[b * LANES : (b + 1) * LANES, :] = spread(total[row : row + 1, :])

                r_copy(d, m).wait_recv()
                value = pbuf[slot, r, :] + rrecv[d, m].astype(F32)

                @pl.when(j >= 2)
                def _():
                    hidden_block(d, j - 2, q, value)

                @pl.when(j == y)
                def _():
                    bown[q] = value

                @pl.when(j == yo)
                def _():
                    bsend[q] = value.astype(BF16)
                    remote(bsend.at[q], bgot.at[q], b_s, b_r, y_peer).start()

    def alone_copy():
        return remote(bsend, bgot, b_s, b_r, y_peer)

    def alone_hidden(q):
        @pl.when(q == 0)
        def _():
            alone_copy().wait_recv()

        for d in range(2):
            @pl.when(place[d] == last)
            def _():
                hidden_block(d, alone, q, bown[q] + bgot[q].astype(F32))

    def early_copy(d, v):
        lower = groups // 2
        ref = hid.at[rows(lax.rem(v, 2) * lower, lower), pl.ds(d * side_rows, side_rows), rows(v // 2 * LANES, LANES)]
        return remote(ref, ref, h_s.at[d], h_r.at[d, lax.rem(v, GATHER_RING)], z_peer[d])

    def late_copy(d, v):
        u = v - 2 * early
        lower = side_rows // 2
        r = rows(d * side_rows + lax.rem(u, 2) * lower, lower)
        ref = hid.at[u // 2, r, pl.ds(early * LANES, (chunks - early) * LANES)]
        return remote(ref, ref, h_s.at[d], h_r.at[d, lax.rem(v, GATHER_RING)], z_peer[d])

    def pass_on(copy, at):
        @pl.when(at > 0)
        def _():
            copy.wait_recv()

        @pl.when(at < last)
        def _():
            copy.start()

    def gather_step(d, i):
        at = place[d]
        v = i - HOP_LAG * at

        @pl.when((v >= 0) & (v < 2 * early))
        def _():
            pass_on(early_copy(d, v), at)

        @pl.when((v >= 2 * early) & (v < gathers))
        def _():
            pass_on(late_copy(d, v), at)

    mine, other = rows(k * side_rows, side_rows), rows((1 - k) * side_rows, side_rows)
    cols_here, cols_there = rows(y * depth, depth), rows(yo * depth, depth)

    def k_copy(g):
        return remote(part.at[g, other, :], kgot.at[g], k_s, k_r.at[lax.rem(g, STAGE_RING)], k_peer)

    def y_copy(g):
        return remote(ysend.at[g], ygot.at[g], y_s, y_r.at[lax.rem(g, STAGE_RING)], y_peer)

    def x_copy(g):
        return remote(xsend.at[g], xgot.at[g], x_s, x_r.at[lax.rem(g, STAGE_RING)], x_peer)

    def g_copy(g):
        ref = branch.at[g, mine, :]
        return remote(ref, ref, g_s, g_r.at[lax.rem(g, STAGE_RING)], k_peer)

    def g_wait(g):
        ref = branch.at[g, other, :]
        remote(ref, ref, g_s, g_r.at[lax.rem(g, STAGE_RING)], k_peer).wait_recv()

    def f_start(b):
        for core, device in enumerate((cb, k_peer[1])):
            for step in range(1 - core, n_ra):
                slot = fgot.at[b, core * (n_ra - 1) + step - 1 + core]
                peer = (lax.rem(ra + step, n_ra), device)
                remote(frow.at[b], slot, f_s.at[b], f_r.at[b], peer).start()

    def f_all(b):
        return remote(fgot.at[b], fgot.at[b], f_s.at[b], f_r.at[b], y_peer)

    def down_product(g):
        value = jnp.dot(hid[g], dwv[...], preferred_element_type=F32)
        part[g] = value.astype(BF16)
        keep[...] = value
        yown[g] = keep[mine, :]
        k_copy(g).start()

    def core_sum(g):
        k_copy(g).wait_recv()
        ysend[g] = (yown[g, :, cols_there] + kgot[g, :, cols_there].astype(F32)).astype(BF16)
        y_copy(g).start()

    def y_sum(g):
        y_copy(g).wait_recv()
        value = yown[g, :, cols_here] + kgot[g, :, cols_here].astype(F32) + ygot[g].astype(F32)
        xsend[g] = value.astype(BF16)
        x_copy(g).start()

    def add_old(g, side):
        r = rows(side * side_rows, side_rows)
        old = tok[rows(side * half + g * side_rows, side_rows), :].astype(F32)
        new = 0.5 * old + branch[g, r, :].astype(F32)
        stream[g, r, :] = new
        return new

    def x_sum(g):
        x_copy(g).wait_recv()
        branch[g, mine, :] = (xsend[g].astype(F32) + xgot[g].astype(F32)).astype(BF16)
        g_copy(g).start()
        new = add_old(g, k)
        b, place_in = g // per_batch, lax.rem(g, per_batch)
        folds[other, :] = jnp.zeros((side_rows, LANES), F32)
        folds[mine, :] = fold(new)
        frow[b, pl.ds(place_in, 1), :] = jnp.sum(jnp.transpose(folds[...]), axis=0, keepdims=True)

        @pl.when(place_in == per_batch - 1)
        def _():
            f_start(b)

    def new_stream(g):
        g_wait(g)
        add_old(g, 1 - k)

    def out_copy(g, side):
        r = rows(side * half + g * side_rows, side_rows)
        return pltpu.make_async_copy(obuf.at[r, :], out.at[r, :], o_s)

    def finish(b):
        f_all(b).wait_recv()
        total = frow[b]
        for r in range(2 * n_ra - 1):
            total = total + fgot[b, r]
        for e in range(per_batch):
            g = b * per_batch + e
            factor = spread(total[e : e + 1, :])
            for side in range(2):
                r = slice(side * side_rows, (side + 1) * side_rows)
                f = factor[r, :]
                to = rows(side * half + g * side_rows, side_rows)
                for c in range(depth // LANES):
                    cols = slice(c * LANES, (c + 1) * LANES)
                    obuf[to, cols] = (stream[g, r, cols] * f * out_gain[:, cols]).astype(BF16)
                out_copy(g, side).start()

    def product(j):
        @pl.when(j == 0)
        def _():
            alone_kept()

        @pl.when(j < 2)
        def _():
            for b in range(nz):
                r = slice(b * block, (b + 1) * block)
                pbuf[j, r, :] = jnp.dot(
                    xf[r, cols_here], wk[alone, rows(j * depth, depth), :], preferred_element_type=F32
                )

        @pl.when(j == 2)
        def _():
            for p in range(PIECES):
                token_wait(1, p)
                token_copy(3, p).start()
            token_quarter(2, kq, yo).wait_recv()
            token_quarter(3, kxq, yo).wait_recv()
            sum_copy().wait()
            srow[...] = srow[...] + speer[...]
            w_kept()

        @pl.when(j >= 2)
        def _():
            w_wait(j - 2)
            for b in range(nz):
                r = slice(b * block, (b + 1) * block)
                pbuf[lax.rem(j, 4), r, :] = jnp.dot(xf[r, :], wk[j - 2], preferred_element_type=F32)

    def tokens_on(p):
        token_wait(0, p)
        token_copy(1, p).start()
        token_copy(2, p).start()

    reduce_end = messages + HOP_LAG * last
    gather_end = messages + gathers + HOP_LAG * last
    ready = messages + 2 * early + HOP_LAG * last + 1
    stages = (down_product, core_sum, y_sum, x_sum, new_stream)
    names = ("down", "core_sum", "y_sum", "x_sum", "new_stream")
    turns = (0,) + STAGE_TURNS
    loop_end = ready + 2 * groups - 1 + turns[-1]

    @pl.loop(0, loop_end)
    def _(i):
        @pl.when((lax.rem(i, STEPS) == 0) & (i < messages))
        def _():
            with jax.named_scope("product"):
                product(i // STEPS)

        for p in range(PIECES):
            @pl.when(i == 2 * p + 3)
            def _():
                with jax.named_scope("tokens"):
                    tokens_on(p)

        @pl.when(i == 2 * STEPS + HOP_LAG * last + 1)
        def _():
            down_send().start()

        @pl.when((i >= messages) & (i < messages + STEPS) & ((z == 0) | (z == last)))
        def _():
            with jax.named_scope("alone"):
                alone_hidden(i - messages)

        @pl.when(i < reduce_end)
        def _():
            with jax.named_scope("reduce"):
                for d in range(2):
                    reduce_step(d, i)

        @pl.when((i >= messages) & (i < gather_end))
        def _():
            with jax.named_scope("gather"):
                for d in range(2):
                    gather_step(d, i - messages)

        def on_turn(offset):
            s = i - ready - offset
            soon = s < 2 * DOWN_LAG
            g = jnp.where(soon, s - DOWN_LAG, s // 2)
            return g, (g >= 0) & (g < groups) & (soon | (lax.rem(s, 2) == 0))

        @pl.when(i >= ready)
        def _():
            @pl.when(i == ready + DOWN_LAG)
            def _():
                with jax.named_scope("down_wait"):
                    down_keep().wait()
                    down_wait()

            for turn, stage, name in reversed(list(zip(turns, stages, names))):
                g, due = on_turn(turn)

                @pl.when(due)
                def _():
                    with jax.named_scope(name):
                        stage(g)

            for b in range(batches - 1):
                g, due = on_turn(turns[-1] + FINISH_LAG)

                @pl.when(due & (g == (b + 1) * per_batch - 1))
                def _():
                    with jax.named_scope("finish"):
                        finish(b)

    with jax.named_scope("drain"):
        for kind, (q, side) in enumerate(((cb, y), (cb, yo), (cb, yo), (xq, yo))):
            token_quarter(kind, q, side).wait_send()
        down_send().wait_send()
        w_sent()

        @pl.when((z == 0) | (z == last))
        def _():
            alone_copy().wait_send()

        for d in range(2):
            @pl.when(place[d] < last)
            def _():
                c_copy(d).wait_send()
                remote(rsend.at[d], rrecv.at[d], r_s.at[d], r_r.at[d, 0], z_peer[d]).wait_send()
                ref = hid.at[:, pl.ds(d * side_rows, side_rows), :]
                remote(ref, ref, h_s.at[d], h_r.at[d, 0], z_peer[d]).wait_send()

        remote(kgot, kgot, k_s, k_r.at[0], k_peer).wait_send()
        remote(ygot, ygot, y_s, y_r.at[0], y_peer).wait_send()
        remote(xgot, xgot, x_s, x_r.at[0], x_peer).wait_send()
        ref = branch.at[:, mine, :]
        remote(ref, ref, g_s, g_r.at[0], k_peer).wait_send()

    with jax.named_scope("finish"):
        finish(batches - 1)
    with jax.named_scope("sent"):
        for b in range(batches):
            f_all(b).wait_send()
        pltpu.make_async_copy(obuf, out, o_s).wait()


def fused_body(nz, ny, n_cb, tokens, norm_gain, gate_weight, up_weight, down_weight, out_gain):
    n_tok, depth = tokens.shape
    n_ra = nz * ny
    units = gate_weight.shape[1] // ny
    chunks = units // LANES
    half = n_tok // 2
    messages = (chunks + 1) * STEPS
    group = n_tok // GROUPS
    side = group // 2
    batches = 2
    dma, vmem = pltpu.SemaphoreType.DMA, pltpu.VMEM
    scratch = [
        vmem((n_tok, ny * depth), BF16),
        vmem((chunks, ny * depth, LANES_PER_STEP), BF16),
        vmem((units, ny * depth), BF16),
        vmem((4, n_tok, LANES_PER_STEP), F32),
        vmem((2, messages, half // STEPS, LANES_PER_STEP), BF16),
        vmem((2, messages, half // STEPS, LANES_PER_STEP), BF16),
        vmem((STEPS, half // STEPS, LANES_PER_STEP), F32),
        vmem((STEPS, half // STEPS, LANES_PER_STEP), BF16),
        vmem((STEPS, half // STEPS, LANES_PER_STEP), BF16),
        vmem((half, LANES), F32),
        vmem((n_tok // LANES, LANES), F32),
        vmem((n_tok // LANES, LANES), F32),
        vmem((2, n_tok // LANES, LANES), F32),
        vmem((2, n_tok // LANES, LANES), F32),
        vmem((GROUPS, group, units), BF16),
        vmem((GROUPS, group, ny * depth), BF16),
        vmem((group, ny * depth), F32),
        vmem((GROUPS, side, ny * depth), BF16),
        vmem((GROUPS, side, ny * depth), F32),
        vmem((GROUPS, side, depth), BF16),
        vmem((GROUPS, side, depth), BF16),
        vmem((GROUPS, side, depth), BF16),
        vmem((GROUPS, side, depth), BF16),
        vmem((GROUPS, group, depth), BF16),
        vmem((GROUPS, group, depth), F32),
        vmem((batches, 8, LANES), F32),
        vmem((batches, 2 * n_ra - 1, 8, LANES), F32),
        dma((4,)), dma((6,)), dma, dma, dma((2,)), dma((2,)),
        dma((2,)), dma, dma((chunks - 1,)), dma, dma, dma, dma, dma,
        dma((2,)), dma((2, RING)), dma((2,)), dma((2, GATHER_RING)),
        dma, dma((STAGE_RING,)), dma, dma((STAGE_RING,)), dma, dma((STAGE_RING,)), dma, dma((STAGE_RING,)),
        dma((batches,)), dma((batches,)), vmem(tokens.shape, BF16), dma, vmem((group, LANES), F32),
        vmem(tokens.shape, BF16), vmem((1, depth), F32), vmem((1, depth), F32), dma((3,)),
    ]
    return pl.pallas_call(
        functools.partial(fused_kernel, nz, ny, n_cb, depth * n_ra),
        out_shape=jax.ShapeDtypeStruct(tokens.shape, BF16),
        in_specs=[pl.BlockSpec(memory_space=pltpu.HBM)] * 6,
        out_specs=pl.BlockSpec(memory_space=pl.ANY),
        scratch_shapes=scratch,
        compiler_params=pltpu.CompilerParams(
            collective_id=0, has_side_effects=True, vmem_limit_bytes=57000 * 1024
        ),
    )(tokens, norm_gain[None, :], gate_weight, up_weight, down_weight, out_gain[None, :])


def solution(mesh):
    n_ra, n_cb = mesh.shape["ra"], mesh.shape["cb"]
    nz, ny = plane_sizes(mesh)
    plain = ring_body(mesh)

    def body(tokens, norm_gain, gate_weight, up_weight, down_weight, out_gain):
        args = (tokens, norm_gain, gate_weight, up_weight, down_weight, out_gain)
        whole = (
            nz == 4 and ny == 2 and n_cb == 4
            and gate_weight.shape[1] % (ny * LANES) == 0
            and tokens.shape[0] == GROUPS * LANES
            and tokens.shape[1] % LANES == 0
        )
        return fused_body(nz, ny, n_cb, *args) if whole else plain(*args)

    placed = (P(None, "ra"), P("ra"), P("ra", "cb"), P("ra", "cb"), P("cb", "ra"), P("ra"))
    return jax.shard_map(body, mesh=mesh, in_specs=placed, out_specs=P(None, "ra"), check_vma=False)
```

```python
import functools

import jax
import jax.numpy as jnp
from jax import lax
from jax.experimental import pallas as pl
from jax.experimental.pallas import tpu as pltpu
from jax.sharding import PartitionSpec as P

F32, BF16 = jnp.float32, jnp.bfloat16
MESH = pl.DeviceIdType.MESH
LANES = 128
LANES_PER_STEP = 2 * LANES
STEPS, GROUPS, PIECES = 4, 8, 2
EARLY_CHUNKS, HOP_LAG, DOWN_LAG = 3, 3, 4
RING, GATHER_RING, STAGE_RING = 16, 12, 8
STAGE_TURNS = (2, 6, 10, 12)
EPS = 1e-06


def plane_sizes(mesh):
    n = mesh.shape["ra"]
    column = mesh.devices[:, 0]
    coords = [getattr(d, "coords", None) for d in column]
    if all(c is not None for c in coords):
        ny = len({c[1] for c in coords})
    else:
        ny = 2 if n % 2 == 0 else 1
    return n // ny, ny


def ring_order(mesh):
    n = mesh.shape["ra"]
    column = mesh.devices[:, 0]
    coords = [getattr(d, "coords", None) for d in column]
    if all(c is not None for c in coords):
        ny = len({c[1] for c in coords})
    else:
        ny = 2 if n % 2 == 0 else 1
    nz = n // ny
    if ny == 1 or nz % 2 or nz * ny != n:
        return list(range(n))
    walk = []
    for z in range(nz):
        ys = range(1, ny) if z % 2 == 0 else range(ny - 1, 0, -1)
        walk += [z * ny + y for y in ys]
    return walk + [z * ny for z in reversed(range(nz))]


def butterfly(value, axis, n, narrow=None):
    if n & (n - 1):
        return lax.psum(value, axis)
    step = 1
    while step < n:
        sent = value if narrow is None else value.astype(narrow)
        got = lax.ppermute(sent, axis, [(i, i ^ step) for i in range(n)])
        value = sent.astype(F32) + got.astype(F32)
        step *= 2
    return value


def ring_body(mesh):
    n_ra, n_cb = mesh.shape["ra"], mesh.shape["cb"]
    order = ring_order(mesh)
    place = [order.index(i) for i in range(n_ra)]
    to_right = [(order[i], order[(i + 1) % n_ra]) for i in range(n_ra)]
    to_left = [(order[i], order[(i - 1) % n_ra]) for i in range(n_ra)]
    far = n_ra // 2

    def body(tokens, norm_gain, gate_weight, up_weight, down_weight, out_gain):
        rows = tokens.shape[0] // n_ra
        width = tokens.shape[1] * n_ra
        hidden_cols = gate_weight.shape[1]
        cut = -(-hidden_cols // 256) * 128
        cols = (slice(0, cut), slice(cut, hidden_cols))
        p = jnp.asarray(place, jnp.int32)[lax.axis_index("ra")]

        def block(array, b):
            start = lax.rem(p + b + n_ra, n_ra) * rows
            return lax.dynamic_slice_in_dim(array, start, rows, 0)

        stream_in = tokens.astype(F32)
        scaled = (stream_in * norm_gain[None, :]).astype(BF16)
        weights = {"g": gate_weight, "u": up_weight}

        def parts(source, offsets):
            x = jnp.concatenate([block(source, b) for b in offsets], axis=0)
            return {k: jnp.dot(x, w, preferred_element_type=F32) for k, w in weights.items()}

        right, left = {}, {}
        source = scaled
        for d in range(far, 0, -1):
            mine = parts(source, (d,) if d == far else (d, -d))
            if d < far:
                source, right["g"] = lax.optimization_barrier((source, right["g"]))
            for key in ("g", "u"):
                for flow, perm, skip, at in ((right, to_right, "u", 0), (left, to_left, "g", rows)):
                    if d == far and key == skip:
                        continue
                    value = mine[key] if d == far else mine[key][at : at + rows]
                    if key in flow:
                        value = value + flow[key].astype(F32)
                    flow[key] = lax.ppermute(value.astype(BF16), "ra", perm)
        mine = parts(source, (0,))

        squares = jnp.sum(stream_in * stream_in, axis=1)
        sq = block(squares, 0)
        for k in range(1, n_ra):
            perm = [(order[i], order[(i + k) % n_ra]) for i in range(n_ra)]
            sq = sq + lax.ppermute(block(squares, k), "ra", perm)
        inv_rms = lax.rsqrt(sq / width + 1e-06)[:, None]

        total = {}
        for key in ("g", "u"):
            value = mine[key]
            for flow in (right, left):
                if key in flow:
                    value = value + flow[key].astype(F32)
            total[key] = value * inv_rms
        own = (jax.nn.silu(total["g"]) * total["u"]).astype(BF16)

        stream = jnp.zeros(tokens.shape, F32)
        sums = jnp.zeros(tokens.shape[:1], F32)

        def finish(stream, sums, held):
            units = jnp.concatenate([h for _, h in held], axis=0)
            down = jnp.dot(units, down_weight, preferred_element_type=F32)
            branch = butterfly(down, "cb", n_cb, BF16)
            for i, (b, _) in enumerate(held):
                new = 0.5 * block(stream_in, b) + branch[i * rows : (i + 1) * rows]
                start = lax.rem(p + b + n_ra, n_ra) * rows
                stream = lax.dynamic_update_slice_in_dim(stream, new, start, 0)
                sums = lax.dynamic_update_slice_in_dim(sums, jnp.sum(new * new, axis=1), start, 0)
            return stream, sums

        from_left = from_right = own
        pending = [(0, own)]
        for s in range(1, far + 1):
            last = s == far
            if last:
                from_left, from_right = from_left[:, cols[0]], from_right[:, cols[1]]
            from_left = lax.ppermute(from_left, "ra", to_right)
            from_right = lax.ppermute(from_right, "ra", to_left)
            stream, sums = finish(stream, sums, pending)
            if last:
                pending = [(far, jnp.concatenate([from_left, from_right], axis=1))]
            else:
                pending = [(-s, from_left), (s, from_right)]
        stream, sums = finish(stream, sums, pending)

        total_sq = butterfly(sums, "ra", n_ra)
        factor = lax.rsqrt(total_sq / width + 1e-06)[:, None]
        return (stream * factor * out_gain[None, :]).astype(BF16)

    return body


def fused_kernel(
    nz, ny, n_cb, width,
    tok_in, gains_in, gate_w, up_w, down_w, out,
    xf, wk, dwv, pbuf, rsend, rrecv, bown, bsend, bgot, inv, srow, speer, csend, crecv, hid,
    part, keep, kgot, yown, ysend, ygot, xsend, xgot, branch, stream, frow, fgot,
    tok_s, tok_r, sum_s, sum_r, c_s, c_r, wl, ws, wr, dl, ds, dr, b_s, b_r, r_s, r_r, h_s, h_r,
    k_s, k_r, y_s, y_r, x_s, x_r, g_s, g_r, f_s, f_r, obuf, o_s, folds, tok, gains, i_s,
):
    arrivals = [
        pltpu.make_async_copy(src, dst, i_s.at[n])
        for n, (src, dst) in enumerate(((tok_in, tok), (gains_in, gains)))
    ]
    for copy in arrivals:
        copy.start()
    n_ra = nz * ny
    tokens, depth = tok.shape
    chunks = wk.shape[0]
    half_cols = chunks * LANES
    half = tokens // 2
    step_rows = half // STEPS
    quarter = tokens // n_cb
    piece_rows = quarter // PIECES
    block = tokens // nz
    alone = chunks - 1
    messages = (chunks + 1) * STEPS
    groups, group, _ = hid.shape
    side_rows = group // 2
    batches = frow.shape[0]
    per_batch = groups // batches
    early = min(EARLY_CHUNKS, chunks - 1)
    gathers = 2 * (early + groups)

    ra, cb = lax.axis_index("ra"), lax.axis_index("cb")
    z, y = ra // ny, ra % ny
    yo = 1 - y
    x, k = cb // 2, cb % 2
    last = nz - 1
    y_peer = (z * ny + yo, cb)
    z_peer = (lax.rem(z + 1, nz) * ny + y, cb), (lax.rem(z + last, nz) * ny + y, cb)
    k_peer = (ra, x * 2 + 1 - k)
    x_peer = (ra, (1 - x) * 2 + k)
    place = (z, last - z)

    def remote(src, dst, send, recv, device):
        return pltpu.make_async_remote_copy(
            src_ref=src, dst_ref=dst, send_sem=send, recv_sem=recv, device_id=device, device_id_type=MESH
        )

    def rows(start, size):
        return pl.ds(pl.multiple_of(start, size), size)

    for side in range(2):
        for i, w in enumerate((gate_w, up_w)):
            cols = pl.ds(side * half_cols + alone * LANES, LANES)
            to = wk.at[alone, pl.ds(side * depth, depth), pl.ds(i * LANES, LANES)]
            pltpu.make_async_copy(w.at[:, cols], to, wl.at[0]).start()

    barrier = pltpu.get_barrier_semaphore()
    for peer in (y_peer, k_peer, x_peer):
        pl.semaphore_signal(barrier, inc=1, device_id=peer, device_id_type=MESH)
    for d in range(2):
        @pl.when(place[d] < last)
        def _():
            pl.semaphore_signal(barrier, inc=1, device_id=z_peer[d], device_id_type=MESH)

    def token_ref(q, p, side):
        return xf.at[rows(q * quarter + p * piece_rows, piece_rows), rows(side * depth, depth)]

    def scale(q, p):
        r = rows(q * quarter + p * piece_rows, piece_rows)
        xf[r, rows(y * depth, depth)] = (tok[r, :].astype(F32) * gains[0:1, :]).astype(BF16)

    xq = lax.rem(cb + 2, n_cb)
    kq = x * 2 + 1 - k
    kxq = (1 - x) * 2 + 1 - k
    token_moves = ((cb, y, y_peer), (cb, yo, x_peer), (cb, yo, k_peer), (xq, yo, k_peer))

    def token_copy(kind, p):
        q, side, device = token_moves[kind]
        recv = tok_r.at[2 * kind + p if kind < 2 else kind + 2]
        return remote(token_ref(q, p, side), token_ref(q, p, side), tok_s.at[kind], recv, device)

    def token_wait(kind, p):
        ref = token_ref((cb, xq)[kind], p, yo)
        remote(ref, ref, tok_s.at[kind], tok_r.at[2 * kind + p], y_peer).wait_recv()

    def token_quarter(kind, q, side):
        ref = xf.at[rows(q * quarter, quarter), rows(side * depth, depth)]
        return remote(ref, ref, tok_s.at[kind], tok_r.at[kind + 2], k_peer)

    def w_slot(j, i, side):
        return wk.at[j, rows(side * depth, depth), pl.ds(i * LANES, LANES)]

    def w_part(j, i, side):
        cols = pl.ds(pl.multiple_of(side * half_cols + j * LANES, LANES), LANES)
        return (gate_w, up_w)[i].at[:, cols]

    def w_send(j, i):
        return remote(w_part(j, i, yo), w_slot(j, i, y), ws, wr.at[j], y_peer)

    def w_sent():
        ref = wk.at[pl.ds(0, alone), rows(y * depth, depth), :]
        remote(ref, ref, ws, wr.at[0], y_peer).wait_send()

    def w_wait(j):
        ref = wk.at[j, rows(yo * depth, depth), :]
        remote(ref, ref, ws, wr.at[j], y_peer).wait_recv()

    def w_kept():
        ref = wk.at[pl.ds(0, alone), rows(y * depth, depth), :]
        pltpu.make_async_copy(ref, ref, wl.at[1]).wait()

    def alone_kept():
        ref = wk.at[alone]
        pltpu.make_async_copy(ref, ref, wl.at[0]).wait()

    def down_rows(side):
        return down_w.at[rows(side * half_cols, half_cols), :]

    down_here = dwv.at[:, rows(y * depth, depth)]
    down_there = dwv.at[:, rows(yo * depth, depth)]

    def down_send():
        return remote(down_rows(yo), down_here, ds, dr, y_peer)

    def down_wait():
        remote(down_there, down_there, ds, dr, y_peer).wait_recv()

    def down_keep():
        return pltpu.make_async_copy(down_rows(y), down_here, dl)

    def fold(value):
        square = value * value
        folded = square[:, :LANES]
        for c in range(1, depth // LANES):
            folded = folded + square[:, c * LANES : (c + 1) * LANES]
        return folded

    def row_sums(value):
        return jnp.sum(jnp.transpose(fold(value)), axis=0, keepdims=True)

    def spread(row):
        return jnp.transpose(jnp.broadcast_to(lax.rsqrt(row / width + EPS), (LANES, LANES)))

    def sum_copy():
        return remote(srow, speer, sum_s, sum_r, y_peer)

    for copy in arrivals:
        copy.wait()
    for p in range(PIECES):
        scale(cb, p)
    pl.semaphore_wait(barrier, 3 + jnp.minimum(z, 1) + jnp.minimum(last - z, 1))
    with jax.named_scope("scale"):
        for p in range(PIECES):
            token_copy(0, p).start()
        for step in range(1, n_cb):
            for p in range(PIECES):
                scale(lax.rem(cb + step, n_cb), p)
    with jax.named_scope("sums"):
        for b in range(tokens // LANES):
            srow[b : b + 1, :] = row_sums(tok[b * LANES : (b + 1) * LANES, :].astype(F32))
        sum_copy().start()
    frow[...] = jnp.zeros_like(frow)

    with jax.named_scope("issue"):
        @pl.loop(0, alone)
        def _(j):
            for i in range(2):
                w_send(j, i).start()

        @pl.loop(0, alone)
        def _(j):
            for i in range(2):
                pltpu.make_async_copy(w_part(j, i, y), w_slot(j, i, y), wl.at[1]).start()

        down_keep().start()

    def r_copy(d, m):
        return remote(rsend.at[d, m], rrecv.at[d, m], r_s.at[d], r_r.at[d, lax.rem(m, RING)], z_peer[d])

    def c_copy(d):
        return remote(csend.at[d], crecv.at[d], c_s.at[d], c_r.at[d], z_peer[d])

    def hidden_block(d, j, q, value):
        factor = inv[rows(q * step_rows, step_rows), :]
        gate = value[:, :LANES] * factor
        up = value[:, LANES:] * factor
        hidden = (gate / (1.0 + jnp.exp(-gate)) * up).astype(BF16)
        per = step_rows // side_rows
        for s in range(per):
            cols = rows(j * LANES, LANES)
            hid[q * per + s, pl.ds((1 - d) * side_rows, side_rows), cols] = hidden[s * side_rows : (s + 1) * side_rows]

    def reduce_step(d, i):
        at = place[d]
        m = i - HOP_LAG * at
        start = (1 - d) * half

        @pl.when((m >= 0) & (m < messages))
        def _():
            j, q = m // STEPS, lax.rem(m, STEPS)
            slot = lax.rem(j, 4)
            r = rows(start + q * step_rows, step_rows)

            @pl.when(at == 0)
            def _():
                @pl.when(m == 2 * STEPS)
                def _():
                    csend[d] = srow[...]
                    c_copy(d).start()

                rsend[d, m] = pbuf[slot, r, :].astype(BF16)
                r_copy(d, m).start()

            @pl.when((at > 0) & (at < last))
            def _():
                @pl.when(m == 2 * STEPS)
                def _():
                    c_copy(d).wait_recv()
                    csend[d] = srow[...] + crecv[d]
                    c_copy(d).start()

                r_copy(d, m).wait_recv()
                rsend[d, m] = (pbuf[slot, r, :] + rrecv[d, m].astype(F32)).astype(BF16)
                r_copy(d, m).start()

            @pl.when(at == last)
            def _():
                @pl.when(m == 2 * STEPS)
                def _():
                    c_copy(d).wait_recv()
                    total = srow[...] + crecv[d]
                    for b in range(half // LANES):
                        row = start // LANES + b
                        inv[b * LANES : (b + 1) * LANES, :] = spread(total[row : row + 1, :])

                r_copy(d, m).wait_recv()
                value = pbuf[slot, r, :] + rrecv[d, m].astype(F32)

                @pl.when(j >= 2)
                def _():
                    hidden_block(d, j - 2, q, value)

                @pl.when(j == y)
                def _():
                    bown[q] = value

                @pl.when(j == yo)
                def _():
                    bsend[q] = value.astype(BF16)
                    remote(bsend.at[q], bgot.at[q], b_s, b_r, y_peer).start()

    def alone_copy():
        return remote(bsend, bgot, b_s, b_r, y_peer)

    def alone_hidden(q):
        @pl.when(q == 0)
        def _():
            alone_copy().wait_recv()

        for d in range(2):
            @pl.when(place[d] == last)
            def _():
                hidden_block(d, alone, q, bown[q] + bgot[q].astype(F32))

    def early_copy(d, v):
        lower = groups // 2
        ref = hid.at[rows(lax.rem(v, 2) * lower, lower), pl.ds(d * side_rows, side_rows), rows(v // 2 * LANES, LANES)]
        return remote(ref, ref, h_s.at[d], h_r.at[d, lax.rem(v, GATHER_RING)], z_peer[d])

    def late_copy(d, v):
        u = v - 2 * early
        lower = side_rows // 2
        r = rows(d * side_rows + lax.rem(u, 2) * lower, lower)
        ref = hid.at[u // 2, r, pl.ds(early * LANES, (chunks - early) * LANES)]
        return remote(ref, ref, h_s.at[d], h_r.at[d, lax.rem(v, GATHER_RING)], z_peer[d])

    def pass_on(copy, at):
        @pl.when(at > 0)
        def _():
            copy.wait_recv()

        @pl.when(at < last)
        def _():
            copy.start()

    def gather_step(d, i):
        at = place[d]
        v = i - HOP_LAG * at

        @pl.when((v >= 0) & (v < 2 * early))
        def _():
            pass_on(early_copy(d, v), at)

        @pl.when((v >= 2 * early) & (v < gathers))
        def _():
            pass_on(late_copy(d, v), at)

    mine, other = rows(k * side_rows, side_rows), rows((1 - k) * side_rows, side_rows)
    cols_here, cols_there = rows(y * depth, depth), rows(yo * depth, depth)

    def k_copy(g):
        return remote(part.at[g, other, :], kgot.at[g], k_s, k_r.at[lax.rem(g, STAGE_RING)], k_peer)

    def y_copy(g):
        return remote(ysend.at[g], ygot.at[g], y_s, y_r.at[lax.rem(g, STAGE_RING)], y_peer)

    def x_copy(g):
        return remote(xsend.at[g], xgot.at[g], x_s, x_r.at[lax.rem(g, STAGE_RING)], x_peer)

    def g_copy(g):
        ref = branch.at[g, mine, :]
        return remote(ref, ref, g_s, g_r.at[lax.rem(g, STAGE_RING)], k_peer)

    def g_wait(g):
        ref = branch.at[g, other, :]
        remote(ref, ref, g_s, g_r.at[lax.rem(g, STAGE_RING)], k_peer).wait_recv()

    def f_start(b):
        for core, device in enumerate((cb, k_peer[1])):
            for step in range(1 - core, n_ra):
                slot = fgot.at[b, core * (n_ra - 1) + step - 1 + core]
                peer = (lax.rem(ra + step, n_ra), device)
                remote(frow.at[b], slot, f_s.at[b], f_r.at[b], peer).start()

    def f_all(b):
        return remote(fgot.at[b], fgot.at[b], f_s.at[b], f_r.at[b], y_peer)

    def down_product(g):
        value = jnp.dot(hid[g], dwv[...], preferred_element_type=F32)
        part[g] = value.astype(BF16)
        keep[...] = value
        yown[g] = keep[mine, :]
        k_copy(g).start()

    def core_sum(g):
        k_copy(g).wait_recv()
        ysend[g] = (yown[g, :, cols_there] + kgot[g, :, cols_there].astype(F32)).astype(BF16)
        y_copy(g).start()

    def y_sum(g):
        y_copy(g).wait_recv()
        value = yown[g, :, cols_here] + kgot[g, :, cols_here].astype(F32) + ygot[g].astype(F32)
        xsend[g] = value.astype(BF16)
        x_copy(g).start()

    def add_old(g, side):
        r = rows(side * side_rows, side_rows)
        old = tok[rows(side * half + g * side_rows, side_rows), :].astype(F32)
        new = 0.5 * old + branch[g, r, :].astype(F32)
        stream[g, r, :] = new
        return new

    def x_sum(g):
        x_copy(g).wait_recv()
        branch[g, mine, :] = (xsend[g].astype(F32) + xgot[g].astype(F32)).astype(BF16)
        g_copy(g).start()
        new = add_old(g, k)
        b, place_in = g // per_batch, lax.rem(g, per_batch)
        folds[other, :] = jnp.zeros((side_rows, LANES), F32)
        folds[mine, :] = fold(new)
        frow[b, pl.ds(place_in, 1), :] = jnp.sum(jnp.transpose(folds[...]), axis=0, keepdims=True)

        @pl.when(place_in == per_batch - 1)
        def _():
            f_start(b)

    def new_stream(g):
        g_wait(g)
        add_old(g, 1 - k)

    def out_copy(g, side):
        r = rows(side * half + g * side_rows, side_rows)
        return pltpu.make_async_copy(obuf.at[r, :], out.at[r, :], o_s)

    def finish(b):
        f_all(b).wait_recv()
        total = frow[b]
        for r in range(2 * n_ra - 1):
            total = total + fgot[b, r]
        for e in range(per_batch):
            g = b * per_batch + e
            factor = spread(total[e : e + 1, :])
            for side in range(2):
                r = slice(side * side_rows, (side + 1) * side_rows)
                f = factor[r, :]
                to = rows(side * half + g * side_rows, side_rows)
                for c in range(depth // LANES):
                    cols = slice(c * LANES, (c + 1) * LANES)
                    obuf[to, cols] = (stream[g, r, cols] * f * gains[1:2, cols]).astype(BF16)
                out_copy(g, side).start()

    def product(j):
        @pl.when(j == 0)
        def _():
            alone_kept()

        @pl.when(j < 2)
        def _():
            for b in range(nz):
                r = slice(b * block, (b + 1) * block)
                pbuf[j, r, :] = jnp.dot(
                    xf[r, cols_here], wk[alone, rows(j * depth, depth), :], preferred_element_type=F32
                )

        @pl.when(j == 2)
        def _():
            for p in range(PIECES):
                token_wait(1, p)
                token_copy(3, p).start()
            token_quarter(2, kq, yo).wait_recv()
            token_quarter(3, kxq, yo).wait_recv()
            sum_copy().wait()
            srow[...] = srow[...] + speer[...]
            w_kept()

        @pl.when(j >= 2)
        def _():
            w_wait(j - 2)
            for b in range(nz):
                r = slice(b * block, (b + 1) * block)
                pbuf[lax.rem(j, 4), r, :] = jnp.dot(xf[r, :], wk[j - 2], preferred_element_type=F32)

    def tokens_on(p):
        token_wait(0, p)
        token_copy(1, p).start()
        token_copy(2, p).start()

    reduce_end = messages + HOP_LAG * last
    gather_end = messages + gathers + HOP_LAG * last
    ready = messages + 2 * early + HOP_LAG * last + 1
    stages = (down_product, core_sum, y_sum, x_sum, new_stream)
    names = ("down", "core_sum", "y_sum", "x_sum", "new_stream")
    turns = (0,) + STAGE_TURNS
    loop_end = ready + 2 * groups - 1 + turns[-1]

    @pl.loop(0, loop_end)
    def _(i):
        @pl.when((lax.rem(i, STEPS) == 0) & (i < messages))
        def _():
            with jax.named_scope("product"):
                product(i // STEPS)

        for p in range(PIECES):
            @pl.when(i == 2 * p + 3)
            def _():
                with jax.named_scope("tokens"):
                    tokens_on(p)

        @pl.when(i == 2 * STEPS + HOP_LAG * last + 1)
        def _():
            down_send().start()

        @pl.when((i >= messages) & (i < messages + STEPS) & ((z == 0) | (z == last)))
        def _():
            with jax.named_scope("alone"):
                alone_hidden(i - messages)

        @pl.when(i < reduce_end)
        def _():
            with jax.named_scope("reduce"):
                for d in range(2):
                    reduce_step(d, i)

        @pl.when((i >= messages) & (i < gather_end))
        def _():
            with jax.named_scope("gather"):
                for d in range(2):
                    gather_step(d, i - messages)

        def on_turn(offset):
            s = i - ready - offset
            soon = s < 2 * DOWN_LAG
            g = jnp.where(soon, s - DOWN_LAG, s // 2)
            return g, (g >= 0) & (g < groups) & (soon | (lax.rem(s, 2) == 0))

        @pl.when(i >= ready)
        def _():
            @pl.when(i == ready + DOWN_LAG)
            def _():
                with jax.named_scope("down_wait"):
                    down_keep().wait()
                    down_wait()

            for turn, stage, name in reversed(list(zip(turns, stages, names))):
                g, due = on_turn(turn)

                @pl.when(due)
                def _():
                    with jax.named_scope(name):
                        stage(g)

    with jax.named_scope("finish"):
        for b in range(batches - 1):
            finish(b)

    with jax.named_scope("drain"):
        for kind, (q, side) in enumerate(((cb, y), (cb, yo), (cb, yo), (xq, yo))):
            token_quarter(kind, q, side).wait_send()
        down_send().wait_send()
        w_sent()

        @pl.when((z == 0) | (z == last))
        def _():
            alone_copy().wait_send()

        for d in range(2):
            @pl.when(place[d] < last)
            def _():
                c_copy(d).wait_send()
                remote(rsend.at[d], rrecv.at[d], r_s.at[d], r_r.at[d, 0], z_peer[d]).wait_send()
                ref = hid.at[:, pl.ds(d * side_rows, side_rows), :]
                remote(ref, ref, h_s.at[d], h_r.at[d, 0], z_peer[d]).wait_send()

        remote(kgot, kgot, k_s, k_r.at[0], k_peer).wait_send()
        remote(ygot, ygot, y_s, y_r.at[0], y_peer).wait_send()
        remote(xgot, xgot, x_s, x_r.at[0], x_peer).wait_send()
        ref = branch.at[:, mine, :]
        remote(ref, ref, g_s, g_r.at[0], k_peer).wait_send()

    with jax.named_scope("finish"):
        finish(batches - 1)
    with jax.named_scope("sent"):
        for b in range(batches):
            f_all(b).wait_send()
        pltpu.make_async_copy(obuf, out, o_s).wait()


def fused_body(nz, ny, n_cb, tokens, norm_gain, gate_weight, up_weight, down_weight, out_gain):
    n_tok, depth = tokens.shape
    n_ra = nz * ny
    units = gate_weight.shape[1] // ny
    chunks = units // LANES
    half = n_tok // 2
    messages = (chunks + 1) * STEPS
    group = n_tok // GROUPS
    side = group // 2
    batches = 2
    dma, vmem = pltpu.SemaphoreType.DMA, pltpu.VMEM
    scratch = [
        vmem((n_tok, ny * depth), BF16),
        vmem((chunks, ny * depth, LANES_PER_STEP), BF16),
        vmem((units, ny * depth), BF16),
        vmem((4, n_tok, LANES_PER_STEP), F32),
        vmem((2, messages, half // STEPS, LANES_PER_STEP), BF16),
        vmem((2, messages, half // STEPS, LANES_PER_STEP), BF16),
        vmem((STEPS, half // STEPS, LANES_PER_STEP), F32),
        vmem((STEPS, half // STEPS, LANES_PER_STEP), BF16),
        vmem((STEPS, half // STEPS, LANES_PER_STEP), BF16),
        vmem((half, LANES), F32),
        vmem((n_tok // LANES, LANES), F32),
        vmem((n_tok // LANES, LANES), F32),
        vmem((2, n_tok // LANES, LANES), F32),
        vmem((2, n_tok // LANES, LANES), F32),
        vmem((GROUPS, group, units), BF16),
        vmem((GROUPS, group, ny * depth), BF16),
        vmem((group, ny * depth), F32),
        vmem((GROUPS, side, ny * depth), BF16),
        vmem((GROUPS, side, ny * depth), F32),
        vmem((GROUPS, side, depth), BF16),
        vmem((GROUPS, side, depth), BF16),
        vmem((GROUPS, side, depth), BF16),
        vmem((GROUPS, side, depth), BF16),
        vmem((GROUPS, group, depth), BF16),
        vmem((GROUPS, group, depth), F32),
        vmem((batches, 8, LANES), F32),
        vmem((batches, 2 * n_ra - 1, 8, LANES), F32),
        dma((4,)), dma((6,)), dma, dma, dma((2,)), dma((2,)),
        dma((2,)), dma, dma((chunks - 1,)), dma, dma, dma, dma, dma,
        dma((2,)), dma((2, RING)), dma((2,)), dma((2, GATHER_RING)),
        dma, dma((STAGE_RING,)), dma, dma((STAGE_RING,)), dma, dma((STAGE_RING,)), dma, dma((STAGE_RING,)),
        dma((batches,)), dma((batches,)), vmem(tokens.shape, BF16), dma, vmem((group, LANES), F32),
        vmem(tokens.shape, BF16), vmem((2, depth), F32), dma((2,)),
    ]
    return pl.pallas_call(
        functools.partial(fused_kernel, nz, ny, n_cb, depth * n_ra),
        out_shape=jax.ShapeDtypeStruct(tokens.shape, BF16),
        in_specs=[pl.BlockSpec(memory_space=pltpu.HBM)] * 5,
        out_specs=pl.BlockSpec(memory_space=pl.ANY),
        scratch_shapes=scratch,
        compiler_params=pltpu.CompilerParams(
            collective_id=0, has_side_effects=True, vmem_limit_bytes=54000 * 1024
        ),
    )(tokens, jnp.stack([norm_gain, out_gain]), gate_weight, up_weight, down_weight)


def solution(mesh):
    n_ra, n_cb = mesh.shape["ra"], mesh.shape["cb"]
    nz, ny = plane_sizes(mesh)
    plain = ring_body(mesh)

    def body(tokens, norm_gain, gate_weight, up_weight, down_weight, out_gain):
        args = (tokens, norm_gain, gate_weight, up_weight, down_weight, out_gain)
        whole = (
            nz == 4 and ny == 2 and n_cb == 4
            and gate_weight.shape[1] % (ny * LANES) == 0
            and tokens.shape[0] == GROUPS * LANES
            and tokens.shape[1] % LANES == 0
        )
        return fused_body(nz, ny, n_cb, *args) if whole else plain(*args)

    placed = (P(None, "ra"), P("ra"), P("ra", "cb"), P("ra", "cb"), P("cb", "ra"), P("ra"))
    return jax.shard_map(body, mesh=mesh, in_specs=placed, out_specs=P(None, "ra"), check_vma=False)
```

```python
import functools

import jax
import jax.numpy as jnp
from jax import lax
from jax.experimental import pallas as pl
from jax.experimental.pallas import tpu as pltpu
from jax.sharding import PartitionSpec as P

F32, BF16 = jnp.float32, jnp.bfloat16
MESH = pl.DeviceIdType.MESH
LANES = 128
LANES_PER_STEP = 2 * LANES
STEPS, GROUPS, PIECES = 4, 8, 2
EARLY_CHUNKS, HOP_LAG, DOWN_LAG = 3, 3, 4
RING, GATHER_RING, STAGE_RING = 16, 12, 8
STAGE_TURNS = (2, 6, 10, 18)
EPS = 1e-06


def plane_sizes(mesh):
    n = mesh.shape["ra"]
    column = mesh.devices[:, 0]
    coords = [getattr(d, "coords", None) for d in column]
    if all(c is not None for c in coords):
        ny = len({c[1] for c in coords})
    else:
        ny = 2 if n % 2 == 0 else 1
    return n // ny, ny


def ring_order(mesh):
    n = mesh.shape["ra"]
    column = mesh.devices[:, 0]
    coords = [getattr(d, "coords", None) for d in column]
    if all(c is not None for c in coords):
        ny = len({c[1] for c in coords})
    else:
        ny = 2 if n % 2 == 0 else 1
    nz = n // ny
    if ny == 1 or nz % 2 or nz * ny != n:
        return list(range(n))
    walk = []
    for z in range(nz):
        ys = range(1, ny) if z % 2 == 0 else range(ny - 1, 0, -1)
        walk += [z * ny + y for y in ys]
    return walk + [z * ny for z in reversed(range(nz))]


def butterfly(value, axis, n, narrow=None):
    if n & (n - 1):
        return lax.psum(value, axis)
    step = 1
    while step < n:
        sent = value if narrow is None else value.astype(narrow)
        got = lax.ppermute(sent, axis, [(i, i ^ step) for i in range(n)])
        value = sent.astype(F32) + got.astype(F32)
        step *= 2
    return value


def ring_body(mesh):
    n_ra, n_cb = mesh.shape["ra"], mesh.shape["cb"]
    order = ring_order(mesh)
    place = [order.index(i) for i in range(n_ra)]
    to_right = [(order[i], order[(i + 1) % n_ra]) for i in range(n_ra)]
    to_left = [(order[i], order[(i - 1) % n_ra]) for i in range(n_ra)]
    far = n_ra // 2

    def body(tokens, norm_gain, gate_weight, up_weight, down_weight, out_gain):
        rows = tokens.shape[0] // n_ra
        width = tokens.shape[1] * n_ra
        hidden_cols = gate_weight.shape[1]
        cut = -(-hidden_cols // 256) * 128
        cols = (slice(0, cut), slice(cut, hidden_cols))
        p = jnp.asarray(place, jnp.int32)[lax.axis_index("ra")]

        def block(array, b):
            start = lax.rem(p + b + n_ra, n_ra) * rows
            return lax.dynamic_slice_in_dim(array, start, rows, 0)

        stream_in = tokens.astype(F32)
        scaled = (stream_in * norm_gain[None, :]).astype(BF16)
        weights = {"g": gate_weight, "u": up_weight}

        def parts(source, offsets):
            x = jnp.concatenate([block(source, b) for b in offsets], axis=0)
            return {k: jnp.dot(x, w, preferred_element_type=F32) for k, w in weights.items()}

        right, left = {}, {}
        source = scaled
        for d in range(far, 0, -1):
            mine = parts(source, (d,) if d == far else (d, -d))
            if d < far:
                source, right["g"] = lax.optimization_barrier((source, right["g"]))
            for key in ("g", "u"):
                for flow, perm, skip, at in ((right, to_right, "u", 0), (left, to_left, "g", rows)):
                    if d == far and key == skip:
                        continue
                    value = mine[key] if d == far else mine[key][at : at + rows]
                    if key in flow:
                        value = value + flow[key].astype(F32)
                    flow[key] = lax.ppermute(value.astype(BF16), "ra", perm)
        mine = parts(source, (0,))

        squares = jnp.sum(stream_in * stream_in, axis=1)
        sq = block(squares, 0)
        for k in range(1, n_ra):
            perm = [(order[i], order[(i + k) % n_ra]) for i in range(n_ra)]
            sq = sq + lax.ppermute(block(squares, k), "ra", perm)
        inv_rms = lax.rsqrt(sq / width + 1e-06)[:, None]

        total = {}
        for key in ("g", "u"):
            value = mine[key]
            for flow in (right, left):
                if key in flow:
                    value = value + flow[key].astype(F32)
            total[key] = value * inv_rms
        own = (jax.nn.silu(total["g"]) * total["u"]).astype(BF16)

        stream = jnp.zeros(tokens.shape, F32)
        sums = jnp.zeros(tokens.shape[:1], F32)

        def finish(stream, sums, held):
            units = jnp.concatenate([h for _, h in held], axis=0)
            down = jnp.dot(units, down_weight, preferred_element_type=F32)
            branch = butterfly(down, "cb", n_cb, BF16)
            for i, (b, _) in enumerate(held):
                new = 0.5 * block(stream_in, b) + branch[i * rows : (i + 1) * rows]
                start = lax.rem(p + b + n_ra, n_ra) * rows
                stream = lax.dynamic_update_slice_in_dim(stream, new, start, 0)
                sums = lax.dynamic_update_slice_in_dim(sums, jnp.sum(new * new, axis=1), start, 0)
            return stream, sums

        from_left = from_right = own
        pending = [(0, own)]
        for s in range(1, far + 1):
            last = s == far
            if last:
                from_left, from_right = from_left[:, cols[0]], from_right[:, cols[1]]
            from_left = lax.ppermute(from_left, "ra", to_right)
            from_right = lax.ppermute(from_right, "ra", to_left)
            stream, sums = finish(stream, sums, pending)
            if last:
                pending = [(far, jnp.concatenate([from_left, from_right], axis=1))]
            else:
                pending = [(-s, from_left), (s, from_right)]
        stream, sums = finish(stream, sums, pending)

        total_sq = butterfly(sums, "ra", n_ra)
        factor = lax.rsqrt(total_sq / width + 1e-06)[:, None]
        return (stream * factor * out_gain[None, :]).astype(BF16)

    return body


def fused_kernel(
    nz, ny, n_cb, width,
    tok_in, gains_in, gate_w, up_w, down_w, out,
    xf, wk, dwv, pbuf, rsend, rrecv, bown, bsend, bgot, inv, srow, speer, csend, crecv, hid,
    part, keep, kgot, yown, ysend, ygot, xsend, xgot, branch, stream, frow, fgot,
    tok_s, tok_r, sum_s, sum_r, c_s, c_r, wl, ws, wr, dl, ds, dr, b_s, b_r, r_s, r_r, h_s, h_r,
    k_s, k_r, y_s, y_r, x_s, x_r, g_s, g_r, f_s, f_r, obuf, o_s, folds, tok, gains, i_s,
):
    arrivals = [
        pltpu.make_async_copy(src, dst, i_s.at[n])
        for n, (src, dst) in enumerate(((tok_in, tok), (gains_in, gains)))
    ]
    for copy in arrivals:
        copy.start()
    n_ra = nz * ny
    tokens, depth = tok.shape
    chunks = wk.shape[0]
    half_cols = chunks * LANES
    half = tokens // 2
    step_rows = half // STEPS
    quarter = tokens // n_cb
    piece_rows = quarter // PIECES
    block = tokens // nz
    alone = chunks - 1
    messages = (chunks + 1) * STEPS
    groups, group, _ = hid.shape
    side_rows = group // 2
    batches = frow.shape[0]
    per_batch = groups // batches
    early = min(EARLY_CHUNKS, chunks - 1)
    gathers = 2 * (early + groups)

    ra, cb = lax.axis_index("ra"), lax.axis_index("cb")
    z, y = ra // ny, ra % ny
    yo = 1 - y
    x, k = cb // 2, cb % 2
    last = nz - 1
    y_peer = (z * ny + yo, cb)
    z_peer = (lax.rem(z + 1, nz) * ny + y, cb), (lax.rem(z + last, nz) * ny + y, cb)
    k_peer = (ra, x * 2 + 1 - k)
    x_peer = (ra, (1 - x) * 2 + k)
    place = (z, last - z)

    def remote(src, dst, send, recv, device):
        return pltpu.make_async_remote_copy(
            src_ref=src, dst_ref=dst, send_sem=send, recv_sem=recv, device_id=device, device_id_type=MESH
        )

    def rows(start, size):
        return pl.ds(pl.multiple_of(start, size), size)

    for side in range(2):
        for i, w in enumerate((gate_w, up_w)):
            cols = pl.ds(side * half_cols + alone * LANES, LANES)
            to = wk.at[alone, pl.ds(side * depth, depth), pl.ds(i * LANES, LANES)]
            pltpu.make_async_copy(w.at[:, cols], to, wl.at[0]).start()

    barrier = pltpu.get_barrier_semaphore()
    for peer in (y_peer, k_peer, x_peer):
        pl.semaphore_signal(barrier, inc=1, device_id=peer, device_id_type=MESH)
    for d in range(2):
        @pl.when(place[d] < last)
        def _():
            pl.semaphore_signal(barrier, inc=1, device_id=z_peer[d], device_id_type=MESH)

    def token_ref(q, p, side):
        return xf.at[rows(q * quarter + p * piece_rows, piece_rows), rows(side * depth, depth)]

    def scale(q, p):
        r = rows(q * quarter + p * piece_rows, piece_rows)
        xf[r, rows(y * depth, depth)] = (tok[r, :].astype(F32) * gains[0:1, :]).astype(BF16)

    xq = lax.rem(cb + 2, n_cb)
    kq = x * 2 + 1 - k
    kxq = (1 - x) * 2 + 1 - k
    token_moves = ((cb, y, y_peer), (cb, yo, x_peer), (cb, yo, k_peer), (xq, yo, k_peer))

    def token_copy(kind, p):
        q, side, device = token_moves[kind]
        recv = tok_r.at[2 * kind + p if kind < 2 else kind + 2]
        return remote(token_ref(q, p, side), token_ref(q, p, side), tok_s.at[kind], recv, device)

    def token_wait(kind, p):
        ref = token_ref((cb, xq)[kind], p, yo)
        remote(ref, ref, tok_s.at[kind], tok_r.at[2 * kind + p], y_peer).wait_recv()

    def token_quarter(kind, q, side):
        ref = xf.at[rows(q * quarter, quarter), rows(side * depth, depth)]
        return remote(ref, ref, tok_s.at[kind], tok_r.at[kind + 2], k_peer)

    def w_slot(j, i, side):
        return wk.at[j, rows(side * depth, depth), pl.ds(i * LANES, LANES)]

    def w_part(j, i, side):
        cols = pl.ds(pl.multiple_of(side * half_cols + j * LANES, LANES), LANES)
        return (gate_w, up_w)[i].at[:, cols]

    def w_send(j, i):
        return remote(w_part(j, i, yo), w_slot(j, i, y), ws, wr.at[j], y_peer)

    def w_sent():
        ref = wk.at[pl.ds(0, alone), rows(y * depth, depth), :]
        remote(ref, ref, ws, wr.at[0], y_peer).wait_send()

    def w_wait(j):
        ref = wk.at[j, rows(yo * depth, depth), :]
        remote(ref, ref, ws, wr.at[j], y_peer).wait_recv()

    def w_kept():
        ref = wk.at[pl.ds(0, alone), rows(y * depth, depth), :]
        pltpu.make_async_copy(ref, ref, wl.at[1]).wait()

    def alone_kept():
        ref = wk.at[alone]
        pltpu.make_async_copy(ref, ref, wl.at[0]).wait()

    def down_rows(side):
        return down_w.at[rows(side * half_cols, half_cols), :]

    down_here = dwv.at[:, rows(y * depth, depth)]
    down_there = dwv.at[:, rows(yo * depth, depth)]

    def down_send():
        return remote(down_rows(yo), down_here, ds, dr, y_peer)

    def down_wait():
        remote(down_there, down_there, ds, dr, y_peer).wait_recv()

    def down_keep():
        return pltpu.make_async_copy(down_rows(y), down_here, dl)

    def fold(value):
        square = value * value
        folded = square[:, :LANES]
        for c in range(1, depth // LANES):
            folded = folded + square[:, c * LANES : (c + 1) * LANES]
        return folded

    def row_sums(value):
        return jnp.sum(jnp.transpose(fold(value)), axis=0, keepdims=True)

    def spread(row):
        return jnp.transpose(jnp.broadcast_to(lax.rsqrt(row / width + EPS), (LANES, LANES)))

    def sum_copy():
        return remote(srow, speer, sum_s, sum_r, y_peer)

    for copy in arrivals:
        copy.wait()
    for p in range(PIECES):
        scale(cb, p)
    pl.semaphore_wait(barrier, 3 + jnp.minimum(z, 1) + jnp.minimum(last - z, 1))
    with jax.named_scope("scale"):
        for p in range(PIECES):
            token_copy(0, p).start()
        for step in range(1, n_cb):
            for p in range(PIECES):
                scale(lax.rem(cb + step, n_cb), p)
    with jax.named_scope("sums"):
        for b in range(tokens // LANES):
            srow[b : b + 1, :] = row_sums(tok[b * LANES : (b + 1) * LANES, :].astype(F32))
        sum_copy().start()
    frow[...] = jnp.zeros_like(frow)

    with jax.named_scope("issue"):
        @pl.loop(0, alone)
        def _(j):
            for i in range(2):
                w_send(j, i).start()

        @pl.loop(0, alone)
        def _(j):
            for i in range(2):
                pltpu.make_async_copy(w_part(j, i, y), w_slot(j, i, y), wl.at[1]).start()

        down_keep().start()

    def r_copy(d, m):
        return remote(rsend.at[d, m], rrecv.at[d, m], r_s.at[d], r_r.at[d, lax.rem(m, RING)], z_peer[d])

    def c_copy(d):
        return remote(csend.at[d], crecv.at[d], c_s.at[d], c_r.at[d], z_peer[d])

    def hidden_block(d, j, q, value):
        factor = inv[rows(q * step_rows, step_rows), :]
        gate = value[:, :LANES] * factor
        up = value[:, LANES:] * factor
        hidden = (gate / (1.0 + jnp.exp(-gate)) * up).astype(BF16)
        per = step_rows // side_rows
        for s in range(per):
            cols = rows(j * LANES, LANES)
            hid[q * per + s, pl.ds((1 - d) * side_rows, side_rows), cols] = hidden[s * side_rows : (s + 1) * side_rows]

    def reduce_step(d, i):
        at = place[d]
        m = i - HOP_LAG * at
        start = (1 - d) * half

        @pl.when((m >= 0) & (m < messages))
        def _():
            j, q = m // STEPS, lax.rem(m, STEPS)
            slot = lax.rem(j, 4)
            r = rows(start + q * step_rows, step_rows)

            @pl.when(at == 0)
            def _():
                @pl.when(m == 2 * STEPS)
                def _():
                    csend[d] = srow[...]
                    c_copy(d).start()

                rsend[d, m] = pbuf[slot, r, :].astype(BF16)
                r_copy(d, m).start()

            @pl.when((at > 0) & (at < last))
            def _():
                @pl.when(m == 2 * STEPS)
                def _():
                    c_copy(d).wait_recv()
                    csend[d] = srow[...] + crecv[d]
                    c_copy(d).start()

                r_copy(d, m).wait_recv()
                rsend[d, m] = (pbuf[slot, r, :] + rrecv[d, m].astype(F32)).astype(BF16)
                r_copy(d, m).start()

            @pl.when(at == last)
            def _():
                @pl.when(m == 2 * STEPS)
                def _():
                    c_copy(d).wait_recv()
                    total = srow[...] + crecv[d]
                    for b in range(half // LANES):
                        row = start // LANES + b
                        inv[b * LANES : (b + 1) * LANES, :] = spread(total[row : row + 1, :])

                r_copy(d, m).wait_recv()
                value = pbuf[slot, r, :] + rrecv[d, m].astype(F32)

                @pl.when(j >= 2)
                def _():
                    hidden_block(d, j - 2, q, value)

                @pl.when(j == y)
                def _():
                    bown[q] = value

                @pl.when(j == yo)
                def _():
                    bsend[q] = value.astype(BF16)
                    remote(bsend.at[q], bgot.at[q], b_s, b_r, y_peer).start()

    def alone_copy():
        return remote(bsend, bgot, b_s, b_r, y_peer)

    def alone_hidden(q):
        @pl.when(q == 0)
        def _():
            alone_copy().wait_recv()

        for d in range(2):
            @pl.when(place[d] == last)
            def _():
                hidden_block(d, alone, q, bown[q] + bgot[q].astype(F32))

    def early_copy(d, v):
        lower = groups // 2
        ref = hid.at[rows(lax.rem(v, 2) * lower, lower), pl.ds(d * side_rows, side_rows), rows(v // 2 * LANES, LANES)]
        return remote(ref, ref, h_s.at[d], h_r.at[d, lax.rem(v, GATHER_RING)], z_peer[d])

    def late_copy(d, v):
        u = v - 2 * early
        lower = side_rows // 2
        r = rows(d * side_rows + lax.rem(u, 2) * lower, lower)
        ref = hid.at[u // 2, r, pl.ds(early * LANES, (chunks - early) * LANES)]
        return remote(ref, ref, h_s.at[d], h_r.at[d, lax.rem(v, GATHER_RING)], z_peer[d])

    def pass_on(copy, at):
        @pl.when(at > 0)
        def _():
            copy.wait_recv()

        @pl.when(at < last)
        def _():
            copy.start()

    def gather_step(d, i):
        at = place[d]
        v = i - HOP_LAG * at

        @pl.when((v >= 0) & (v < 2 * early))
        def _():
            pass_on(early_copy(d, v), at)

        @pl.when((v >= 2 * early) & (v < gathers))
        def _():
            pass_on(late_copy(d, v), at)

    mine, other = rows(k * side_rows, side_rows), rows((1 - k) * side_rows, side_rows)
    cols_here, cols_there = rows(y * depth, depth), rows(yo * depth, depth)

    def k_copy(g):
        return remote(part.at[g, other, :], kgot.at[g], k_s, k_r.at[lax.rem(g, STAGE_RING)], k_peer)

    def y_copy(g):
        return remote(ysend.at[g], ygot.at[g], y_s, y_r.at[lax.rem(g, STAGE_RING)], y_peer)

    def x_copy(g):
        return remote(xsend.at[g], xgot.at[g], x_s, x_r.at[lax.rem(g, STAGE_RING)], x_peer)

    def g_copy(g):
        ref = branch.at[g, mine, :]
        return remote(ref, ref, g_s, g_r.at[lax.rem(g, STAGE_RING)], k_peer)

    def g_wait(g):
        ref = branch.at[g, other, :]
        remote(ref, ref, g_s, g_r.at[lax.rem(g, STAGE_RING)], k_peer).wait_recv()

    def f_start(b):
        for core, device in enumerate((cb, k_peer[1])):
            for step in range(1 - core, n_ra):
                slot = fgot.at[b, core * (n_ra - 1) + step - 1 + core]
                peer = (lax.rem(ra + step, n_ra), device)
                remote(frow.at[b], slot, f_s.at[b], f_r.at[b], peer).start()

    def f_all(b):
        return remote(fgot.at[b], fgot.at[b], f_s.at[b], f_r.at[b], y_peer)

    def down_product(g):
        value = jnp.dot(hid[g], dwv[...], preferred_element_type=F32)
        part[g] = value.astype(BF16)
        keep[...] = value
        yown[g] = keep[mine, :]
        k_copy(g).start()

    def core_sum(g):
        k_copy(g).wait_recv()
        ysend[g] = (yown[g, :, cols_there] + kgot[g, :, cols_there].astype(F32)).astype(BF16)
        y_copy(g).start()

    def y_sum(g):
        y_copy(g).wait_recv()
        value = yown[g, :, cols_here] + kgot[g, :, cols_here].astype(F32) + ygot[g].astype(F32)
        xsend[g] = value.astype(BF16)
        x_copy(g).start()

    def add_old(g, side):
        r = rows(side * side_rows, side_rows)
        old = tok[rows(side * half + g * side_rows, side_rows), :].astype(F32)
        new = 0.5 * old + branch[g, r, :].astype(F32)
        stream[g, r, :] = new
        return new

    def x_sum(g):
        x_copy(g).wait_recv()
        branch[g, mine, :] = (xsend[g].astype(F32) + xgot[g].astype(F32)).astype(BF16)
        g_copy(g).start()
        new = add_old(g, k)
        b, place_in = g // per_batch, lax.rem(g, per_batch)
        folds[other, :] = jnp.zeros((side_rows, LANES), F32)
        folds[mine, :] = fold(new)
        frow[b, pl.ds(place_in, 1), :] = jnp.sum(jnp.transpose(folds[...]), axis=0, keepdims=True)

        @pl.when(place_in == per_batch - 1)
        def _():
            f_start(b)

    def new_stream(g):
        g_wait(g)
        add_old(g, 1 - k)

    def out_copy(g, side):
        r = rows(side * half + g * side_rows, side_rows)
        return pltpu.make_async_copy(obuf.at[r, :], out.at[r, :], o_s)

    def finish(b):
        f_all(b).wait_recv()
        total = frow[b]
        for r in range(2 * n_ra - 1):
            total = total + fgot[b, r]
        for e in range(per_batch):
            g = b * per_batch + e
            factor = spread(total[e : e + 1, :])
            for side in range(2):
                r = slice(side * side_rows, (side + 1) * side_rows)
                f = factor[r, :]
                to = rows(side * half + g * side_rows, side_rows)
                for c in range(depth // LANES):
                    cols = slice(c * LANES, (c + 1) * LANES)
                    obuf[to, cols] = (stream[g, r, cols] * f * gains[1:2, cols]).astype(BF16)
                out_copy(g, side).start()

    def product(j):
        @pl.when(j == 0)
        def _():
            alone_kept()

        @pl.when(j < 2)
        def _():
            for b in range(nz):
                r = slice(b * block, (b + 1) * block)
                pbuf[j, r, :] = jnp.dot(
                    xf[r, cols_here], wk[alone, rows(j * depth, depth), :], preferred_element_type=F32
                )

        @pl.when(j == 2)
        def _():
            for p in range(PIECES):
                token_wait(1, p)
                token_copy(3, p).start()
            token_quarter(2, kq, yo).wait_recv()
            token_quarter(3, kxq, yo).wait_recv()
            sum_copy().wait()
            srow[...] = srow[...] + speer[...]
            w_kept()

        @pl.when(j >= 2)
        def _():
            w_wait(j - 2)
            for b in range(nz):
                r = slice(b * block, (b + 1) * block)
                pbuf[lax.rem(j, 4), r, :] = jnp.dot(xf[r, :], wk[j - 2], preferred_element_type=F32)

    def tokens_on(p):
        token_wait(0, p)
        token_copy(1, p).start()
        token_copy(2, p).start()

    reduce_end = messages + HOP_LAG * last
    gather_end = messages + gathers + HOP_LAG * last
    ready = messages + 2 * early + HOP_LAG * last + 1
    stages = (down_product, core_sum, y_sum, x_sum, new_stream)
    names = ("down", "core_sum", "y_sum", "x_sum", "new_stream")
    turns = (0,) + STAGE_TURNS
    loop_end = ready + 2 * groups - 1 + turns[-1]

    @pl.loop(0, loop_end)
    def _(i):
        @pl.when((lax.rem(i, STEPS) == 0) & (i < messages))
        def _():
            with jax.named_scope("product"):
                product(i // STEPS)

        for p in range(PIECES):
            @pl.when(i == 2 * p + 3)
            def _():
                with jax.named_scope("tokens"):
                    tokens_on(p)

        @pl.when(i == 2 * STEPS + HOP_LAG * last + 1)
        def _():
            down_send().start()

        @pl.when((i >= messages) & (i < messages + STEPS) & ((z == 0) | (z == last)))
        def _():
            with jax.named_scope("alone"):
                alone_hidden(i - messages)

        @pl.when(i < reduce_end)
        def _():
            with jax.named_scope("reduce"):
                for d in range(2):
                    reduce_step(d, i)

        @pl.when((i >= messages) & (i < gather_end))
        def _():
            with jax.named_scope("gather"):
                for d in range(2):
                    gather_step(d, i - messages)

        def on_turn(offset):
            s = i - ready - offset
            soon = s < 2 * DOWN_LAG
            g = jnp.where(soon, s - DOWN_LAG, s // 2)
            return g, (g >= 0) & (g < groups) & (soon | (lax.rem(s, 2) == 0))

        @pl.when(i >= ready)
        def _():
            @pl.when(i == ready + DOWN_LAG)
            def _():
                with jax.named_scope("down_wait"):
                    down_keep().wait()
                    down_wait()

            for turn, stage, name in reversed(list(zip(turns, stages, names))):
                g, due = on_turn(turn)

                @pl.when(due)
                def _():
                    with jax.named_scope(name):
                        stage(g)

    with jax.named_scope("finish"):
        for b in range(batches - 1):
            finish(b)

    with jax.named_scope("drain"):
        for kind, (q, side) in enumerate(((cb, y), (cb, yo), (cb, yo), (xq, yo))):
            token_quarter(kind, q, side).wait_send()
        down_send().wait_send()
        w_sent()

        @pl.when((z == 0) | (z == last))
        def _():
            alone_copy().wait_send()

        for d in range(2):
            @pl.when(place[d] < last)
            def _():
                c_copy(d).wait_send()
                remote(rsend.at[d], rrecv.at[d], r_s.at[d], r_r.at[d, 0], z_peer[d]).wait_send()
                ref = hid.at[:, pl.ds(d * side_rows, side_rows), :]
                remote(ref, ref, h_s.at[d], h_r.at[d, 0], z_peer[d]).wait_send()

        remote(kgot, kgot, k_s, k_r.at[0], k_peer).wait_send()
        remote(ygot, ygot, y_s, y_r.at[0], y_peer).wait_send()
        remote(xgot, xgot, x_s, x_r.at[0], x_peer).wait_send()
        ref = branch.at[:, mine, :]
        remote(ref, ref, g_s, g_r.at[0], k_peer).wait_send()

    with jax.named_scope("finish"):
        finish(batches - 1)
    with jax.named_scope("sent"):
        for b in range(batches):
            f_all(b).wait_send()
        pltpu.make_async_copy(obuf, out, o_s).wait()


def fused_body(nz, ny, n_cb, tokens, norm_gain, gate_weight, up_weight, down_weight, out_gain):
    n_tok, depth = tokens.shape
    n_ra = nz * ny
    units = gate_weight.shape[1] // ny
    chunks = units // LANES
    half = n_tok // 2
    messages = (chunks + 1) * STEPS
    group = n_tok // GROUPS
    side = group // 2
    batches = 2
    dma, vmem = pltpu.SemaphoreType.DMA, pltpu.VMEM
    scratch = [
        vmem((n_tok, ny * depth), BF16),
        vmem((chunks, ny * depth, LANES_PER_STEP), BF16),
        vmem((units, ny * depth), BF16),
        vmem((4, n_tok, LANES_PER_STEP), F32),
        vmem((2, messages, half // STEPS, LANES_PER_STEP), BF16),
        vmem((2, messages, half // STEPS, LANES_PER_STEP), BF16),
        vmem((STEPS, half // STEPS, LANES_PER_STEP), F32),
        vmem((STEPS, half // STEPS, LANES_PER_STEP), BF16),
        vmem((STEPS, half // STEPS, LANES_PER_STEP), BF16),
        vmem((half, LANES), F32),
        vmem((n_tok // LANES, LANES), F32),
        vmem((n_tok // LANES, LANES), F32),
        vmem((2, n_tok // LANES, LANES), F32),
        vmem((2, n_tok // LANES, LANES), F32),
        vmem((GROUPS, group, units), BF16),
        vmem((GROUPS, group, ny * depth), BF16),
        vmem((group, ny * depth), F32),
        vmem((GROUPS, side, ny * depth), BF16),
        vmem((GROUPS, side, ny * depth), F32),
        vmem((GROUPS, side, depth), BF16),
        vmem((GROUPS, side, depth), BF16),
        vmem((GROUPS, side, depth), BF16),
        vmem((GROUPS, side, depth), BF16),
        vmem((GROUPS, group, depth), BF16),
        vmem((GROUPS, group, depth), F32),
        vmem((batches, 8, LANES), F32),
        vmem((batches, 2 * n_ra - 1, 8, LANES), F32),
        dma((4,)), dma((6,)), dma, dma, dma((2,)), dma((2,)),
        dma((2,)), dma, dma((chunks - 1,)), dma, dma, dma, dma, dma,
        dma((2,)), dma((2, RING)), dma((2,)), dma((2, GATHER_RING)),
        dma, dma((STAGE_RING,)), dma, dma((STAGE_RING,)), dma, dma((STAGE_RING,)), dma, dma((STAGE_RING,)),
        dma((batches,)), dma((batches,)), vmem(tokens.shape, BF16), dma, vmem((group, LANES), F32),
        vmem(tokens.shape, BF16), vmem((2, depth), F32), dma((2,)),
    ]
    return pl.pallas_call(
        functools.partial(fused_kernel, nz, ny, n_cb, depth * n_ra),
        out_shape=jax.ShapeDtypeStruct(tokens.shape, BF16),
        in_specs=[pl.BlockSpec(memory_space=pltpu.HBM)] * 5,
        out_specs=pl.BlockSpec(memory_space=pl.ANY),
        scratch_shapes=scratch,
        compiler_params=pltpu.CompilerParams(
            collective_id=0, has_side_effects=True, vmem_limit_bytes=54000 * 1024
        ),
    )(tokens, jnp.stack([norm_gain, out_gain]), gate_weight, up_weight, down_weight)


def solution(mesh):
    n_ra, n_cb = mesh.shape["ra"], mesh.shape["cb"]
    nz, ny = plane_sizes(mesh)
    plain = ring_body(mesh)

    def body(tokens, norm_gain, gate_weight, up_weight, down_weight, out_gain):
        args = (tokens, norm_gain, gate_weight, up_weight, down_weight, out_gain)
        whole = (
            nz == 4 and ny == 2 and n_cb == 4
            and gate_weight.shape[1] % (ny * LANES) == 0
            and tokens.shape[0] == GROUPS * LANES
            and tokens.shape[1] % LANES == 0
        )
        return fused_body(nz, ny, n_cb, *args) if whole else plain(*args)

    placed = (P(None, "ra"), P("ra"), P("ra", "cb"), P("ra", "cb"), P("cb", "ra"), P("ra"))
    return jax.shard_map(body, mesh=mesh, in_specs=placed, out_specs=P(None, "ra"), check_vma=False)
```
